256 devices in a mesh: grp: 2 (over y), sp: 32 (over z, core), tp: 4 (over x).
Axes of the slice: x: 4, y: 2, z: 16, core: 2. Of those that a mesh axis runs over, the one named last changes fastest.
The devices are a block of a 4x16x16 slice.
Arguments:
- receptance: bfloat16 [8192, 512], P(('grp', 'sp'), 'tp'), parts along dimension 0, may hold values from -6 to 6
- key_matrix: bfloat16 [8192, 512], P(('grp', 'sp'), 'tp'), parts along dimension 0, may hold values from -6 to 6
- value_matrix: bfloat16 [8192, 512], P(('grp', 'sp'), 'tp'), parts along dimension 0, may hold values from -6 to 6
- output_gate_logits: bfloat16 [8192, 512], P(('grp', 'sp'), 'tp'), parts along dimension 0, may hold values from -6 to 6
- onward_decay_logits: bfloat16 [8192, 512], P(('grp', 'sp'), 'tp'), parts along dimension 0, may hold values from -14 to 3
- reverse_decay_logits: bfloat16 [8192, 512], P(('grp', 'sp'), 'tp'), parts along dimension 0, may hold values from -14 to 3
- correction_rate_logits: bfloat16 [8192, 512], P(('grp', 'sp'), 'tp'), parts along dimension 0, may hold values from -12 to 5
- extra_log_decay: float32 [8192, 8], P(('grp', 'sp'), 'tp'), parts along dimension 0, may hold values from -0.7 to 0
- documents: int32 [8192], P(('grp', 'sp')), parts along dimension 0, may hold values from 0 to 7, never falling along the last dimension, each value on 1 to 2048 neighbouring positions
- head_norm_scale: float32 [512], P('tp'), may hold values from 0.1 to 1.9
- mixer_output_weight: bfloat16 [512, 2048], P('tp'), may hold values from -0.25 to 0.25
- residual: bfloat16 [8192, 2048], P(('grp', 'sp', 'tp')), parts along dimension 0, may hold values from -6 to 6
- expert_norm_scale: float32 [2048], replicated, may hold values from 0.1 to 1.9
- expert_choice_index: int32 [8192, 2], P(('grp', 'sp', 'tp')), parts along dimension 0, may hold values from 0 to 127, as said below
- group_route_weight: float32 [8192], P(('grp', 'sp', 'tp')), parts along dimension 0, may hold values from 0.2 to 1
- expert_route_weight: float32 [8192, 2], P(('grp', 'sp', 'tp')), parts along dimension 0, may hold values from 0.05 to 1
- expert_gate_matrix: bfloat16 [128, 2048, 512], P(('sp', 'tp')), may hold values from -0.125 to 0.125
- expert_up_matrix: bfloat16 [128, 2048, 512], P(('sp', 'tp')), may hold values from -0.125 to 0.125
- expert_down_matrix: bfloat16 [128, 512, 2048], P(('sp', 'tp')), may hold values from -0.25 to 0.25
Outputs:
- updated: bfloat16 [8192, 2048], P(('grp', 'sp', 'tp')), parts along dimension 0
The draws below stay inside these ranges and needn't reach their ends.
There are 2 independent parts, one for each index of `grp`. The reference program is written for one: setup_inputs(seed, part) draws one part's arguments, and reference() takes and returns one part's arrays. A program takes and returns all parts, laid end to end along the dimension named above; an argument that names none is the same for every part. Nothing has to cross between parts.
Inputs may be any that keep to these rules, and one draw needn't show every extreme that they name: `expert_choice_index`: each row names two different experts of one group (experts g * 4 to g * 4 + 3). In each aligned block of 32 rows no expert is named more than 2 times, and one expert is named exactly 2 times in every block.
All inputs are finite; a program needn't handle non-finite values.
Results may differ from the reference program's by a relative error of at most 0.012.
Values may be sent and summed in bfloat16 or wider, within the bound.
A program may use at most 64 MiB of HBM per device.

```python
import math
import jax
import jax.numpy as jnp
import numpy as np
from jax import lax

D = 2048
HEADS = 8
HEAD_DIM = 64
D_EXPERT = 512
EXP_GROUP = 4
TOK_DEV = 128
WIDTH = 512
TOKENS = 4096
MOE_ROWS = 32
EXPERTS = 128
CAP = 2
SEG_COUNT = 8
SEG_MOST = 2048


def slow_heads(key):
    share = 0.5
    return jax.random.uniform(jax.random.fold_in(key, 7001), (HEADS,)) < share


def head_field(key, salt, slow_value, fast_value, spread):
    slow = slow_heads(key)
    base = jnp.repeat(jnp.where(slow, slow_value, fast_value), HEAD_DIM)
    channel = 0.3 * jax.random.normal(jax.random.fold_in(key, salt + 1), (WIDTH,))
    noise = spread * jax.random.normal(jax.random.fold_in(key, salt + 2), (TOKENS, WIDTH))
    blocks = TOKENS // TOK_DEV
    factor = jax.random.uniform(jax.random.fold_in(key, salt + 3), (blocks, 1, HEADS), minval=-0.7, maxval=0.7)
    factor = jnp.broadcast_to(factor, (blocks, TOK_DEV, HEADS)).reshape(TOKENS, HEADS)
    factor = jnp.repeat(factor, HEAD_DIM, axis=1)
    return base[None, :] + channel[None, :] + noise + factor


def draw_onward_decay_logits(key, part):
    return jnp.clip(head_field(key, 100, -9.5, -3.0, 1.0), -14.0, 3.0).astype(jnp.bfloat16)


def draw_reverse_decay_logits(key, part):
    return jnp.clip(head_field(key, 200, -9.5, -3.0, 1.0), -14.0, 3.0).astype(jnp.bfloat16)


def draw_correction_rate_logits(key, part):
    return jnp.clip(head_field(key, 300, -7.0, 0.0, 1.2), -12.0, 5.0).astype(jnp.bfloat16)


def draw_extra_log_decay(key, part):
    struck = jax.random.uniform(jax.random.fold_in(key, 401), (TOKENS, HEADS)) < 6.0 / TOKENS
    kept = jax.random.uniform(jax.random.fold_in(key, 402), (TOKENS, HEADS), minval=0.5, maxval=0.8)
    return jnp.where(struck, jnp.log(kept), 0.0).astype(jnp.float32)


def draw_expert_choice_index(key, part):
    groups = EXPERTS // EXP_GROUP
    blocks = TOKENS // MOE_ROWS
    hot_expert = jax.random.randint(jax.random.fold_in(key, 501), (), 0, EXPERTS)
    hot_group = hot_expert // EXP_GROUP
    turn_index = jnp.arange(CAP)
    partner = hot_group * EXP_GROUP + (hot_expert % EXP_GROUP + 1 + turn_index % (EXP_GROUP - 1)) % EXP_GROUP
    hot_rows = jnp.stack([jnp.full((CAP,), hot_expert), partner], axis=1)
    slot_count = (groups - 1) * 2 * CAP
    slot_index = jnp.arange(slot_count)
    offset = slot_index // (2 * CAP)
    group_index = offset + (offset >= hot_group).astype(jnp.int32)
    pair_side = slot_index % 2

    def one_block(block_key):
        block_keys = jax.random.split(block_key, 3)
        scores = jax.random.randint(block_keys[0], (groups, EXP_GROUP), 0, 1 << 20) * EXP_GROUP + jnp.arange(EXP_GROUP)
        ordering = jnp.argsort(scores, axis=1, stable=True)
        leading = ordering[group_index, 2 * pair_side]
        trailing = ordering[group_index, 2 * pair_side + 1]
        pairs = jnp.stack([group_index * EXP_GROUP + leading, group_index * EXP_GROUP + trailing], axis=1)
        chosen = pairs[jax.random.permutation(block_keys[1], slot_count)[:MOE_ROWS - CAP]]
        block_rows = jnp.concatenate([hot_rows, chosen], axis=0)
        return block_rows[jax.random.permutation(block_keys[2], MOE_ROWS)]
    all_rows = jax.vmap(one_block)(jax.random.split(jax.random.fold_in(key, 502), blocks))
    return all_rows.reshape(TOKENS, 2).astype(jnp.int32)


def levels(own_key, shape, cuts, least, largest):
    loudness = 1.0
    for position, shards_of in cuts:
        draws = jax.random.uniform(jax.random.fold_in(jax.random.fold_in(own_key, 6), position), (shards_of,), jnp.float32, least / len(cuts), largest / len(cuts))
        loudness = loudness * jnp.repeat(jnp.exp(draws), shape[position] // shards_of).reshape((-1,) + (1,) * (len(shape) - 1 - position))
    return loudness


def split_up(count, total, most, slope):
    loads = [(1 << 20) // math.isqrt(rank ** slope) + 1 for rank in range(2, count + 1)]
    spare, given = total - most - (count - 1), [1] * (count - 1)
    while spare > 0:
        free = [i for i in range(count - 1) if given[i] < most]
        mass, remaining = sum([loads[i] for i in free]), spare
        for i in free:
            more = min(most - given[i], max(1, remaining * loads[i] // mass), spare)
            given[i] = given[i] + more
            spare = spare - more
    return np.array([most] + given)


def ragged_sizes(rng, amount, total, bound, lean):
    if amount == 2:
        one = jax.random.randint(rng, (), max(1, total - bound), min(bound, total - 1) + 1)
        return jnp.stack([one, total - one])
    tallies = jnp.asarray(split_up(amount, total, bound, lean), jnp.int32)
    couples = (amount - 1) // 2
    source_of, receiver = tallies[1:1 + 2 * couples:2], tallies[2:2 + 2 * couples:2]
    margin = jnp.minimum(source_of - 1, bound - receiver)
    moved = jax.random.randint(jax.random.fold_in(rng, 1), (couples,), 0, 1 << 20) % (margin + 1)
    tallies = tallies.at[1:1 + 2 * couples:2].set(source_of - moved).at[2:2 + 2 * couples:2].set(receiver + moved)
    return tallies[jax.random.permutation(jax.random.fold_in(rng, 2), amount)]


def scatter_about(own_key, dims, deviation, most, pieces=(), kind=jnp.bfloat16):
    result = deviation * jax.random.normal(own_key, dims, jnp.float32)
    if pieces:
        result = result * levels(own_key, dims, pieces, -0.22, 0.18)
    return jnp.clip(result, -most, most).astype(kind)


def setup_inputs(seed: int = 0, part: int = 0) -> dict:
    seeds = jax.random.split(jax.random.key(seed), 20)
    part_splits = jax.random.split(jax.random.fold_in(seeds[19], part), 20)
    return {
        "receptance": scatter_about(part_splits[0], (TOKENS, WIDTH), 1.0, 6.0, ((0, 32), (1, 4))),
        "key_matrix": scatter_about(part_splits[1], (TOKENS, WIDTH), 1.0, 6.0, ((0, 32), (1, 4))),
        "value_matrix": scatter_about(part_splits[2], (TOKENS, WIDTH), 1.0, 6.0, ((0, 32), (1, 4))),
        "output_gate_logits": scatter_about(part_splits[3], (TOKENS, WIDTH), 1.0, 6.0, ((0, 32), (1, 4))),
        "onward_decay_logits": draw_onward_decay_logits(jax.random.fold_in(jax.random.fold_in(seeds[19], part), 71), part),
        "reverse_decay_logits": draw_reverse_decay_logits(jax.random.fold_in(jax.random.fold_in(seeds[19], part), 71), part),
        "correction_rate_logits": draw_correction_rate_logits(jax.random.fold_in(jax.random.fold_in(seeds[19], part), 71), part),
        "extra_log_decay": draw_extra_log_decay(jax.random.fold_in(jax.random.fold_in(seeds[19], part), 71), part),
        "documents": jnp.searchsorted(jnp.cumsum(ragged_sizes(part_splits[8], SEG_COUNT, TOKENS, SEG_MOST, 0)), jnp.arange(TOKENS), side="right").astype(jnp.int32),
        "head_norm_scale": jnp.clip(1.0 + 0.18 * jax.random.normal(seeds[9], (WIDTH,), jnp.float32), 0.1, 1.9),
        "mixer_output_weight": scatter_about(seeds[10], (WIDTH, D), WIDTH ** -0.5, 0.25, ((0, 4),)),
        "residual": scatter_about(part_splits[11], (TOKENS, D), 1.0, 6.0, ((0, 128),)),
        "expert_norm_scale": jnp.clip(1.0 + 0.18 * jax.random.normal(seeds[12], (D,), jnp.float32), 0.1, 1.9),
        "expert_choice_index": draw_expert_choice_index(jax.random.fold_in(jax.random.fold_in(seeds[19], part), 71), part),
        "group_route_weight": jnp.clip(0.2 + 0.8 * jax.random.uniform(part_splits[14], (TOKENS,), jnp.float32) ** levels(part_splits[14], (TOKENS,), ((0, 128),), -0.2, 0.2), 0.2, 1.0),
        "expert_route_weight": jnp.clip(0.05 + 0.95 * jax.random.uniform(part_splits[15], (TOKENS, 2), jnp.float32) ** levels(part_splits[15], (TOKENS, 2), ((0, 128),), -0.2, 0.2), 0.05, 1.0),
        "expert_gate_matrix": scatter_about(seeds[16], (EXPERTS, D, D_EXPERT), D ** -0.5, 0.125, ((0, 128),)),
        "expert_up_matrix": scatter_about(seeds[17], (EXPERTS, D, D_EXPERT), D ** -0.5, 0.125, ((0, 128),)),
        "expert_down_matrix": scatter_about(seeds[18], (EXPERTS, D_EXPERT, D), D_EXPERT ** -0.5, 0.25, ((0, 128),)),
    }


highest = lax.Precision.HIGHEST

def sweep(reader, key_heads, value_heads, unit_keys, rates, log_decay, documents):
    keep = jnp.concatenate([jnp.zeros((1,), jnp.float32), (documents[1:] == documents[:-1]).astype(jnp.float32)])

    def advance(state, item):
        read_now, key_now, value_now, unit_now, rate_now, decay_now, keep_now = item
        state = state * keep_now
        along = jnp.einsum('hvk,hk->hv', state, unit_now, precision=highest)
        state = state * jnp.exp(decay_now)[:, None, :] - along[:, :, None] * (rate_now * unit_now)[:, None, :] + value_now[:, :, None] * key_now[:, None, :]
        return (state, jnp.einsum('hvk,hk->hv', state, read_now, precision=highest))
    start = jnp.zeros((HEADS, HEAD_DIM, HEAD_DIM), jnp.float32)
    _, outputs = lax.scan(advance, start, (reader, key_heads, value_heads, unit_keys, rates, log_decay, keep))
    return outputs

def reference(receptance, key_matrix, value_matrix, output_gate_logits, onward_decay_logits, reverse_decay_logits, correction_rate_logits, extra_log_decay, documents, head_norm_scale, mixer_output_weight, residual, expert_norm_scale, expert_choice_index, group_route_weight, expert_route_weight, expert_gate_matrix, expert_up_matrix, expert_down_matrix):
    length = receptance.shape[0]
    triple_shape3 = (length, HEADS, HEAD_DIM)
    reader = receptance.astype(jnp.float32).reshape(triple_shape3)
    key_heads = key_matrix.astype(jnp.float32).reshape(triple_shape3)
    value_heads = value_matrix.astype(jnp.float32).reshape(triple_shape3)
    unit_keys = key_heads * lax.rsqrt(lax.optimization_barrier(jnp.sum(key_heads * key_heads, axis=-1, keepdims=True)) + 1e-06)
    rates = jax.nn.sigmoid(correction_rate_logits.astype(jnp.float32)).reshape(triple_shape3)
    decay_spike = extra_log_decay[:, :, None]
    onward_log_decay = -jnp.exp(-jax.nn.softplus(-onward_decay_logits.astype(jnp.float32)) - 0.5).reshape(triple_shape3) + decay_spike
    reverse_log_decay = -jnp.exp(-jax.nn.softplus(-reverse_decay_logits.astype(jnp.float32)) - 0.5).reshape(triple_shape3) + decay_spike
    forward = sweep(reader, key_heads, value_heads, unit_keys, rates, onward_log_decay, documents)
    backward = sweep(reader[::-1], key_heads[::-1], value_heads[::-1], unit_keys[::-1], rates[::-1], reverse_log_decay[::-1], documents[::-1])[::-1]
    total = forward + backward
    centred = total - lax.optimization_barrier(jnp.mean(total, axis=-1, keepdims=True))
    scaled = centred * lax.rsqrt(lax.optimization_barrier(jnp.mean(centred * centred, axis=-1, keepdims=True)) + 0.00064)
    mix = (scaled.reshape(length, WIDTH) * head_norm_scale * jax.nn.sigmoid(output_gate_logits.astype(jnp.float32))).astype(jnp.bfloat16)
    hidden = (residual.astype(jnp.float32) + jnp.dot(mix, mixer_output_weight, preferred_element_type=jnp.float32)).astype(jnp.bfloat16)
    hidden_f = hidden.astype(jnp.float32)
    normed = (hidden_f * lax.rsqrt(lax.optimization_barrier(jnp.mean(hidden_f * hidden_f, axis=-1, keepdims=True)) + 1e-06) * expert_norm_scale).astype(jnp.bfloat16)
    weights = group_route_weight[:, None] * expert_route_weight / lax.optimization_barrier(jnp.sum(expert_route_weight, axis=-1, keepdims=True))
    flat_ids = expert_choice_index.reshape(-1)
    flat_weights = weights.reshape(-1)
    most = EXPERTS * CAP

    def per_expert(carry, expert):
        chosen = flat_ids == expert
        positions = jnp.nonzero(chosen, size=most, fill_value=0)[0].astype(jnp.int32)
        live_mask = (jnp.arange(most, dtype=jnp.int32) < jnp.sum(chosen.astype(jnp.int32))).astype(jnp.float32)
        row_index = positions // 2
        picked = normed[row_index]
        activated = (jax.nn.silu(jnp.dot(picked, expert_gate_matrix[expert], preferred_element_type=jnp.float32)) * jnp.dot(picked, expert_up_matrix[expert], preferred_element_type=jnp.float32)).astype(jnp.bfloat16)
        answer = jnp.dot(activated, expert_down_matrix[expert], preferred_element_type=jnp.float32).astype(jnp.bfloat16)
        scaled_weight = flat_weights[positions] * live_mask
        return (carry.at[row_index].add(answer.astype(jnp.float32) * scaled_weight[:, None]), None)
    combined, _ = lax.scan(per_expert, jnp.zeros((length, D), jnp.float32), jnp.arange(EXPERTS, dtype=jnp.int32))
    return (hidden_f + combined).astype(jnp.bfloat16)
```

```python
import functools

import jax
import jax.numpy as jnp
from jax import lax
from jax.experimental import pallas as pl
from jax.experimental.pallas import tpu as pltpu
from jax.sharding import PartitionSpec as P

HEAD_DIM = 64
GRP_SP = ("grp", "sp")
GRP_SP_TP = ("grp", "sp", "tp")
SP_TP = ("sp", "tp")
MESH = pl.DeviceIdType.MESH
HIGHEST = lax.Precision.HIGHEST
F32 = jnp.float32
BF16 = jnp.bfloat16
QUARTERS = 4
SLOTS = 4
GROUP = 4
CAP = 2
REACH = 4


def dot(a, b, dims=((1,), (0,)), precision=None):
    return lax.dot_general(a, b, (dims, ((), ())), preferred_element_type=F32, precision=precision)


def low(a, b, dims=((1,), (0,))):
    return dot(a.astype(BF16), b.astype(BF16), dims)


ROWS = ((0,), (0,))
LANES = ((1,), (1,))


def iota(shape, dim):
    return lax.broadcasted_iota(jnp.int32, shape, dim)


def sigmoid(x):
    return 1.0 / (1.0 + jnp.exp(-x))


def inverse(lower, row, col):
    eye = (row == col).astype(F32)
    near = jnp.where((row >> 3) == (col >> 3), lower, 0.0)
    second = dot(near, near, precision=HIGHEST)
    fourth = dot(second, second, precision=HIGHEST)
    found = dot(eye - near, eye + second, precision=HIGHEST)
    found = dot(found, eye + fourth, precision=HIGHEST)
    bit = 3
    while (1 << bit) < lower.shape[0]:
        across = ((row >> (bit + 1)) == (col >> (bit + 1))) & ((row >> bit) != (col >> bit))
        found = found - low(low(found, jnp.where(across, lower, 0.0)), found)
        bit += 1
    return found


def column_of(line, eye):
    return jnp.sum(jnp.where(eye, line, jnp.zeros_like(line)), axis=1, keepdims=True)


def line_of(column, eye):
    return jnp.sum(jnp.where(eye, column, jnp.zeros_like(column)), axis=0, keepdims=True)


def direction(reader, keys, values, unit, rates, log_decay, doc_col, doc_row, back):
    n = reader.shape[0]
    row, col = iota((n, n), 0), iota((n, n), 1)
    lane = iota((1, n), 1)
    first_head = lane < HEAD_DIM
    same_head = (row < HEAD_DIM) == (col < HEAD_DIM)
    upto = (col >= row) if back else (col <= row)
    match = doc_col == doc_row
    inclusive = upto & match
    strict = inclusive & (row != col)
    running = dot(upto.astype(F32), log_decay, precision=HIGHEST)
    total = running[:1] if back else running[n - 1 :]
    middle = 0.5 * total
    before = running - log_decay
    head_doc = doc_row[:, n - 1 :] if back else doc_row[:, :1]
    tail_doc = doc_row[:, :1] if back else doc_row[:, n - 1 :]
    opened = (doc_col == head_doc).astype(F32)
    closing = (doc_col == tail_doc).astype(F32)
    probe = unit * jnp.exp(before - middle)
    lifted = reader * jnp.exp(running - middle)
    undo = jnp.exp(middle - running)
    fix_keys = rates * unit * undo
    add_keys = keys * undo
    rest = jnp.exp(total - running)
    fix_last = rates * unit * rest
    add_last = keys * rest
    probe_open = opened * unit * jnp.exp(before)
    lifted_open = opened * reader * jnp.exp(running)
    left = jnp.concatenate([probe, lifted], axis=0)
    right = jnp.concatenate([fix_keys, add_keys], axis=0).astype(BF16)
    values_low = values.astype(BF16)
    removed, added, reads = [], [], []
    for head in range(2):
        mine = first_head if head == 0 else jnp.logical_not(first_head)
        grams = low(jnp.where(mine, left, 0.0), right, LANES)
        system = jnp.where(strict, grams[:n, :n], 0.0)
        add_mix = jnp.where(strict, grams[:n, n:], 0.0)
        reads.append(jnp.where(inclusive, grams[n:, :n], 0.0))
        read_add = jnp.where(inclusive, grams[n:, n:], 0.0)
        mixed = low(jnp.concatenate([add_mix, read_add], axis=0), values_low)
        added.append(mixed[n:])
        source = -jnp.concatenate([mixed[:n], probe_open], axis=1)
        removed.append(low(inverse(system, row, col), source))
    both = jnp.concatenate([first_head, first_head], axis=1)
    took = jnp.where(both, removed[0], removed[1])
    heads = [low(reads[head], took) for head in range(2)]
    through = jnp.where(both, heads[0], heads[1])
    outputs = through[:, :n] + jnp.where(first_head, added[0], added[1])
    response = through[:, n:] + lifted_open
    ends = low(took * closing, fix_last, ROWS)
    add = ends[:n] + low(values * closing, add_last, ROWS)
    whole = (head_doc == tail_doc).astype(F32)
    keep = ends[n:] + jnp.where(row == col, whole * jnp.exp(total), 0.0)
    add = jnp.where(same_head, add, 0.0)
    keep = jnp.where(same_head, keep, 0.0)
    half = n // 2
    element = jnp.concatenate(
        [
            keep[:half] + keep[half:],
            add[:half] + add[half:],
            jnp.broadcast_to(head_doc, (8, n)),
            jnp.broadcast_to(tail_doc, (8, n)),
        ],
        axis=0,
    ).astype(BF16)
    return outputs, response, element


def spread(block, same_head):
    return jnp.where(same_head, jnp.concatenate([block, block], axis=0), jnp.zeros_like(same_head, block.dtype))


def link(tail, head):
    return (tail == head).astype(F32)


def kernel(sizes, *refs):
    (
        receptance_ref, key_ref, value_ref, out_gate_ref, onward_ref, reverse_ref, rate_ref, extra_ref,
        docs_ref, head_scale_ref, mixer_hbm, residual_ref, expert_scale_ref, choice_ref, group_weight_ref,
        route_ref, gate_hbm, up_hbm, down_hbm,
        updated_ref,
        element, partner, chip, near, window, far, entering,
        partial, shares, meta_out, meta_in, packed, arrived, pick, weigh_hi, weigh_lo,
        outward, inbound, answers, answered, combined, returned,
        mixer_w, gate_w, up_w, down_w,
        w_sem, pair_sem, near_send, near_recv, far_sem, tp_send, tp_recv,
        meta_send, meta_recv, out_send, out_recv, x_send, x_recv, y_send, y_recv, back_send, back_recv,
    ) = refs
    SP, TP = sizes
    chips = SP // 2
    sp, tp = lax.axis_index("sp"), lax.axis_index("tp")
    z, core = lax.div(sp, 2), lax.rem(sp, 2)
    n = receptance_ref.shape[0]
    count, width = residual_ref.shape
    quarter = width // QUARTERS
    piece = QUARTERS * SLOTS

    barrier = pltpu.get_barrier_semaphore()

    def greet_sp(o, carry):
        pl.semaphore_signal(barrier, inc=1, device_id={"sp": lax.rem(sp + o, SP)}, device_id_type=MESH)
        return carry

    lax.fori_loop(1, SP, greet_sp, 0)
    for o in range(1, TP):
        pl.semaphore_signal(barrier, inc=1, device_id={"tp": lax.rem(tp + o, TP)}, device_id_type=MESH)

    loads = [
        pltpu.make_async_copy(src, dst, w_sem.at[k])
        for k, (src, dst) in enumerate(
            ((mixer_hbm, mixer_w), (gate_hbm, gate_w), (up_hbm, up_w), (down_hbm, down_w))
        )
    ]
    for load in loads:
        load.start()

    lane32, row32 = iota((count, count), 1), iota((count, count), 0)
    eye32 = lane32 == row32
    choice = choice_ref[...].astype(F32)
    lead, trail = choice[:, :1], choice[:, 1:2]
    lead_group = jnp.floor(lead * (1.0 / GROUP))
    lead_line, trail_line, group_line = (line_of(part, eye32) for part in (lead, trail, lead_group))
    earlier = lane32 < row32

    def rank(mask):
        return jnp.sum(jnp.where(earlier & mask, 1.0, 0.0), axis=1, keepdims=True)

    slot = rank(lead_group == group_line)
    lead_rank = rank((lead == lead_line) | (lead == trail_line))
    trail_rank = rank((trail == lead_line) | (trail == trail_line))
    route = route_ref[...]
    scale = column_of(group_weight_ref[...], eye32) / (route[:, :1] + route[:, 1:2])
    lane = iota((count, 128), 1).astype(F32)
    lead_own, trail_own = lead - GROUP * lead_group, trail - GROUP * lead_group
    info = (
        jnp.where(lane == lead_own, lead_rank + 1.0, 0.0)
        + jnp.where(lane == trail_own, trail_rank + 1.0, 0.0)
        + jnp.where(lane == lead_own + GROUP, scale * route[:, :1], 0.0)
        + jnp.where(lane == trail_own + GROUP, scale * route[:, 1:2], 0.0)
    )
    meta_lane = iota((count, SP * 8), 1)
    meta_pick = (lead_group == (meta_lane >> 3).astype(F32)) & (slot == (meta_lane & 7).astype(F32))
    meta_out[...] = dot(meta_pick.astype(F32).T, info, precision=HIGHEST)
    stacked = QUARTERS * count
    group4, slot4 = jnp.concatenate([lead_group] * QUARTERS, 0), jnp.concatenate([slot] * QUARTERS, 0)
    place = iota((stacked, SP * piece), 1)
    place_row = iota((stacked, SP * piece), 0)
    table_rows = (
        (group4 == (place >> 4).astype(F32))
        & (slot4 == (place & 3).astype(F32))
        & (lax.div(place_row, count) == ((place >> 2) & 3))
    ).astype(F32)

    pl.semaphore_wait(barrier, SP - 1 + TP - 1)

    def sp_copy(src, dst, send, recv, o, rows):
        peer = lax.rem(sp + o, SP)
        return pltpu.make_async_remote_copy(
            src_ref=src.at[pl.ds(pl.multiple_of(peer * rows, rows), rows)],
            dst_ref=dst.at[pl.ds(pl.multiple_of(sp * rows, rows), rows)],
            send_sem=send.at[o],
            recv_sem=recv.at[o],
            device_id={"sp": peer},
            device_id_type=MESH,
        )

    def turn(k):
        half = lax.div(k + 1, 2)
        return SP // 2 + jnp.where(lax.rem(k, 2) == 1, -half, half)

    def start_sp(src, dst, send, recv, rows):
        def one(k, carry):
            sp_copy(src, dst, send, recv, turn(k), rows).start()
            return carry

        lax.fori_loop(0, SP - 1, one, 0)

    def wait_sp(src, dst, send, recv, rows, which):
        def one(o, carry):
            copy = sp_copy(src, dst, send, recv, o, rows)
            copy.wait_send() if which == "send" else copy.wait_recv()
            return carry

        lax.fori_loop(1, SP, one, 0)

    def tp_copy(src, dst, send, recv, o, toward):
        peer = lax.rem(tp + (o if toward else TP - o), TP)
        return pltpu.make_async_remote_copy(
            src_ref=src, dst_ref=dst, send_sem=send.at[o], recv_sem=recv.at[o],
            device_id={"tp": peer}, device_id_type=MESH,
        )

    start_sp(meta_out, meta_in, meta_send, meta_recv, 8)

    row, col = iota((n, n), 0), iota((n, n), 1)
    eye = row == col
    same_head = (row < HEAD_DIM) == (col < HEAD_DIM)
    first_head = iota((1, n), 1) < HEAD_DIM
    doc_row = docs_ref[...].astype(F32)
    doc_col = column_of(doc_row, eye)
    reader = receptance_ref[...].astype(F32)
    keys = key_ref[...].astype(F32)
    values = value_ref[...].astype(F32)

    def by_head(x):
        one = jnp.sum(jnp.where(first_head, x, 0.0), axis=1, keepdims=True)
        two = jnp.sum(jnp.where(first_head, 0.0, x), axis=1, keepdims=True)
        return jnp.where(first_head, one, two)

    unit = keys * lax.rsqrt(by_head(keys * keys) + 1e-06)
    rates = sigmoid(rate_ref[...].astype(F32))
    extra = jnp.where(first_head, extra_ref[:, :1], extra_ref[:, 1:2])
    level = 0.6065306597126334
    onward = -level * sigmoid(onward_ref[...].astype(F32)) + extra
    reverse = -level * sigmoid(reverse_ref[...].astype(F32)) + extra
    out_f, resp_f, element_f = direction(reader, keys, values, unit, rates, onward, doc_col, doc_row, False)
    out_b, resp_b, element_b = direction(reader, keys, values, unit, rates, reverse, doc_col, doc_row, True)
    element[0] = element_f
    element[1] = element_b

    sign = 1 - 2 * core

    def pair_copy(src, dst, k):
        return pltpu.make_async_remote_copy(
            src_ref=src, dst_ref=dst, send_sem=pair_sem.at[2 * k], recv_sem=pair_sem.at[2 * k + 1],
            device_id={"sp": sp + sign}, device_id_type=MESH,
        )

    def chip_peer(distance):
        return lax.rem(z + sign * distance + chips, chips) * 2 + core

    def exists(distance):
        origin = z - sign * distance
        return (origin >= 0) & (origin < chips)

    half = n // 2

    def parts(ref_value):
        value = ref_value.astype(F32)
        return value[:half], value[half : 2 * half], value[n : n + 1], value[n + 8 : n + 9]

    first_copy = pair_copy(element.at[1 - core], partner, 0)
    first_copy.start()
    first_copy.wait()
    own = element[core].astype(F32)
    own_keep, own_add, own_head, own_tail = own[:half], own[half:n], own[n : n + 1], own[n + 8 : n + 9]
    par_keep, par_add, par_head, par_tail = parts(partner[...])
    joined = link(own_tail, par_head)
    both = joined * low(own[:n], spread(par_keep, same_head))
    chip[...] = jnp.concatenate(
        [both[:half], both[half:] + par_add, jnp.broadcast_to(own_head, (8, n)), jnp.broadcast_to(par_tail, (8, n))],
        axis=0,
    ).astype(BF16)

    def near_copy(k):
        return pltpu.make_async_remote_copy(
            src_ref=chip, dst_ref=near.at[k - 1], send_sem=near_send.at[k - 1], recv_sem=near_recv.at[k - 1],
            device_id={"sp": chip_peer(k)}, device_id_type=MESH,
        )

    for k in range(REACH, 0, -1):
        near_copy(k).start()
    for k in range(1, REACH + 1):
        near_copy(k).wait_recv()
    keep, add, win_head, tail = parts(near[REACH - 1])
    tail = jnp.where(exists(REACH), tail, -1.0)
    for k in range(REACH - 1, 0, -1):
        next_keep, next_add, next_head, next_tail = parts(near[k - 1])
        step = link(tail, next_head) * low(
            jnp.concatenate([keep, add], axis=0), spread(next_keep, same_head)
        )
        keep, add = step[:half], step[half:] + next_add
        tail = jnp.where(exists(k), next_tail, -1.0)
    window[...] = jnp.concatenate(
        [add, jnp.broadcast_to(tail, (16, n))], axis=0
    ).astype(BF16)
    far_copy = pltpu.make_async_remote_copy(
        src_ref=window, dst_ref=far, send_sem=far_sem.at[0], recv_sem=far_sem.at[1],
        device_id={"sp": chip_peer(REACH)}, device_id_type=MESH,
    )
    far_copy.start()
    for k in range(1, REACH + 1):
        near_copy(k).wait_send()
    far_copy.wait()
    far_value = far[...].astype(F32)
    far_tail = jnp.where(exists(REACH), far_value[half : half + 1], -1.0)
    add = add + link(far_tail, win_head) * low(far_value[:half], spread(keep, same_head))
    state = link(tail, own_head) * add
    passed = (low(state, spread(own_keep, same_head)) + own_add) * joined
    entering[0] = passed.astype(BF16)
    last_copy = pair_copy(entering.at[0], entering.at[1], 1)
    last_copy.start()
    last_copy.wait()
    other = entering[1].astype(F32)
    state_f = jnp.where(core == 0, state, other)
    state_b = jnp.where(core == 0, other, state)
    entry = jnp.concatenate([spread(state_f, same_head), spread(state_b, same_head)], axis=1)
    mixed = out_f + out_b + low(jnp.concatenate([resp_f, resp_b], axis=1), entry, LANES)

    centred = mixed - by_head(mixed) * (1.0 / HEAD_DIM)
    scaled = centred * lax.rsqrt(by_head(centred * centred) * (1.0 / HEAD_DIM) + 0.00064)
    mix = (scaled * head_scale_ref[...] * sigmoid(out_gate_ref[...].astype(F32))).astype(BF16)
    loads[0].wait()
    partial[...] = dot(mix, mixer_w[...]).astype(BF16)

    def share_copy(o):
        peer = lax.rem(tp + o, TP)
        src = partial.at[pl.ds(pl.multiple_of(peer * count, count), count)]
        return tp_copy(src, shares.at[o], tp_send, tp_recv, o, True)

    for o in (2, 1, 3):
        share_copy(o).start()
    hidden = residual_ref[...].astype(F32)
    own_share = partial[pl.ds(pl.multiple_of(tp * count, count), count)].astype(F32)
    for o in (1, 3, 2):
        share_copy(o).wait_recv()
    shared = own_share + shares[1].astype(F32) + shares[2].astype(F32) + shares[3].astype(F32)
    hidden = (hidden + shared).astype(BF16).astype(F32)
    normed = (
        hidden * lax.rsqrt(jnp.mean(hidden * hidden, axis=1, keepdims=True) + 1e-06) * expert_scale_ref[...]
    ).astype(BF16)

    quarters = jnp.concatenate([normed[:, q * quarter : (q + 1) * quarter] for q in range(QUARTERS)], axis=0)
    packed[...] = dot(table_rows.T.astype(BF16), quarters).astype(BF16)
    start_sp(packed, arrived, out_send, out_recv, piece)
    mine = pl.ds(pl.multiple_of(sp * piece, piece), piece)
    arrived[mine] = packed[mine]

    wait_sp(meta_out, meta_in, meta_send, meta_recv, 8, "recv")
    own_meta = pl.ds(pl.multiple_of(sp * 8, 8), 8)
    meta_in[own_meta] = meta_out[own_meta]
    size = SP * piece
    wide_row, wide_col = iota((size, SP * 8), 0), iota((size, SP * 8), 1)
    widen = ((wide_row >> 4) == (wide_col >> 3)) & ((wide_row & 3) == (wide_col & 7))
    meta = dot(widen.astype(F32), meta_in[...], precision=HIGHEST)
    meta_lane = iota((size, 128), 1)
    taken = SP * CAP
    t_row, t_col = iota((size, taken), 0), iota((size, taken), 1)
    same_source = (t_row >> 4) == (t_col >> 1)
    for o in range(TP):
        expert = lax.rem(tp + o, TP)
        code = jnp.sum(jnp.where(meta_lane == expert, meta, 0.0), axis=1, keepdims=True)
        weight = jnp.sum(jnp.where(meta_lane == expert + GROUP, meta, 0.0), axis=1, keepdims=True)
        hit = same_source & (code == ((t_col & 1) + 1).astype(F32))
        for q in range(QUARTERS):
            here = jnp.where(hit & (((t_row >> 2) & 3) == q), 1.0, 0.0)
            pick[o, q * taken : (q + 1) * taken] = here.T.astype(BF16)
            value = here * weight
            high = value.astype(BF16)
            at = slice((q * TP + o) * taken, (q * TP + o + 1) * taken)
            weigh_hi[o, q] = high
            weigh_lo[o, q] = (value - high.astype(F32)).astype(BF16)
    wait_sp(packed, arrived, out_send, out_recv, piece, "recv")

    def to_expert(o):
        return tp_copy(outward.at[o], inbound.at[o], x_send, x_recv, o, True)

    for o in (2, 1, 3, 0):
        rows = dot(pick[o], arrived[...]).astype(BF16)
        target = inbound if o == 0 else outward
        for q in range(QUARTERS):
            target[o, :, q * quarter : (q + 1) * quarter] = rows[q * taken : (q + 1) * taken]
        if o:
            to_expert(o).start()
    for load in loads[1:]:
        load.wait()
    for o in (1, 3, 2):
        to_expert(o).wait_recv()

    def back_copy(o):
        return tp_copy(answers.at[o], answered.at[o], y_send, y_recv, o, False)

    rows = inbound[...].reshape(TP * taken, width)
    gate = dot(rows, gate_w[...])
    up = dot(rows, up_w[...])
    active = (gate * sigmoid(gate) * up).astype(BF16)
    result = dot(active, down_w[...]).astype(BF16)
    for o in (2, 1, 3, 0):
        target = answered if o == 0 else answers
        target[o] = result[o * taken : (o + 1) * taken]
        if o:
            back_copy(o).start()
    for o in (1, 3, 2):
        back_copy(o).wait_recv()

    total = jnp.zeros((size, quarter), F32)
    for o in range(TP):
        for q in range(QUARTERS):
            answer = answered[o, :, q * quarter : (q + 1) * quarter]
            total += dot(weigh_hi[o, q], answer) + dot(weigh_lo[o, q], answer)
    combined[...] = total.astype(BF16)
    start_sp(combined, returned, back_send, back_recv, piece)
    returned[mine] = combined[mine]
    wait_sp(combined, returned, back_send, back_recv, piece, "recv")
    final = dot(table_rows.astype(BF16), returned[...])
    for q in range(QUARTERS):
        at = slice(q * quarter, (q + 1) * quarter)
        updated_ref[:, at] = (hidden[:, at] + final[q * count : (q + 1) * count]).astype(BF16)

    for o in range(1, TP):
        share_copy(o).wait_send()
        to_expert(o).wait_send()
        back_copy(o).wait_send()
    wait_sp(meta_out, meta_in, meta_send, meta_recv, 8, "send")
    wait_sp(packed, arrived, out_send, out_recv, piece, "send")
    wait_sp(combined, returned, back_send, back_recv, piece, "send")


def solution(mesh):
    SP, TP = mesh.shape["sp"], mesh.shape["tp"]

    def body(
        receptance, key_matrix, value_matrix, output_gate_logits, onward_decay_logits, reverse_decay_logits,
        correction_rate_logits, extra_log_decay, documents, head_norm_scale, mixer_output_weight, residual,
        expert_norm_scale, expert_choice_index, group_route_weight, expert_route_weight,
        expert_gate_matrix, expert_up_matrix, expert_down_matrix,
    ):
        n, channels = receptance.shape
        count, width = residual.shape
        hidden_units = expert_gate_matrix.shape[2]
        piece = QUARTERS * SLOTS
        size, taken, quarter = SP * piece, SP * CAP, width // QUARTERS
        vmem, hbm = pl.BlockSpec(memory_space=pltpu.VMEM), pl.BlockSpec(memory_space=pl.ANY)
        dma = pltpu.SemaphoreType.DMA
        return pl.pallas_call(
            functools.partial(kernel, (SP, TP)),
            out_shape=jax.ShapeDtypeStruct((count, width), BF16),
            in_specs=[vmem] * 10 + [hbm] + [vmem] * 5 + [hbm] * 3,
            out_specs=vmem,
            scratch_shapes=[
                pltpu.VMEM((2, n + 16, n), BF16),
                pltpu.VMEM((n + 16, n), BF16),
                pltpu.VMEM((n + 16, n), BF16),
                pltpu.VMEM((REACH, n + 16, n), BF16),
                pltpu.VMEM((n // 2 + 16, n), BF16),
                pltpu.VMEM((n // 2 + 16, n), BF16),
                pltpu.VMEM((2, n // 2, n), BF16),
                pltpu.VMEM((n, width), BF16),
                pltpu.VMEM((TP, count, width), BF16),
                pltpu.VMEM((SP * 8, 128), F32),
                pltpu.VMEM((SP * 8, 128), F32),
                pltpu.VMEM((size, quarter), BF16),
                pltpu.VMEM((size, quarter), BF16),
                pltpu.VMEM((TP, QUARTERS * taken, size), BF16),
                pltpu.VMEM((TP, QUARTERS, size, taken), BF16),
                pltpu.VMEM((TP, QUARTERS, size, taken), BF16),
                pltpu.VMEM((TP, taken, width), BF16),
                pltpu.VMEM((TP, taken, width), BF16),
                pltpu.VMEM((TP, taken, width), BF16),
                pltpu.VMEM((TP, taken, width), BF16),
                pltpu.VMEM((size, quarter), BF16),
                pltpu.VMEM((size, quarter), BF16),
                pltpu.VMEM((channels, width), BF16),
                pltpu.VMEM((width, hidden_units), BF16),
                pltpu.VMEM((width, hidden_units), BF16),
                pltpu.VMEM((hidden_units, width), BF16),
                dma((4,)), dma((4,)), dma((REACH,)), dma((REACH,)), dma((2,)), dma((TP,)), dma((TP,)),
                dma((SP,)), dma((SP,)), dma((SP,)), dma((SP,)), dma((TP,)), dma((TP,)), dma((TP,)), dma((TP,)),
                dma((SP,)), dma((SP,)),
            ],
            compiler_params=pltpu.CompilerParams(
                collective_id=0, has_side_effects=True, vmem_limit_bytes=56 * 1024 * 1024
            ),
        )(
            receptance, key_matrix, value_matrix, output_gate_logits, onward_decay_logits, reverse_decay_logits,
            correction_rate_logits, extra_log_decay, documents.reshape(1, n), head_norm_scale.reshape(1, channels),
            mixer_output_weight, residual, expert_norm_scale.reshape(1, width), expert_choice_index,
            group_route_weight.reshape(1, count), expert_route_weight,
            expert_gate_matrix[0], expert_up_matrix[0], expert_down_matrix[0],
        )

    in_specs = (
        (P(GRP_SP, "tp"),) * 8
        + (P(GRP_SP), P("tp"), P("tp", None), P(GRP_SP_TP, None), P(), P(GRP_SP_TP, None))
        + (P(GRP_SP_TP), P(GRP_SP_TP, None))
        + (P(SP_TP, None, None),) * 3
    )
    return jax.shard_map(
        body, mesh=mesh, in_specs=in_specs, out_specs=P(GRP_SP_TP, None), check_vma=False
    )
```

```python
import functools

import jax
import jax.numpy as jnp
from jax import lax
from jax.experimental import pallas as pl
from jax.experimental.pallas import tpu as pltpu
from jax.sharding import PartitionSpec as P

HEAD_DIM = 64
GRP_SP = ("grp", "sp")
GRP_SP_TP = ("grp", "sp", "tp")
SP_TP = ("sp", "tp")
MESH = pl.DeviceIdType.MESH
HIGHEST = lax.Precision.HIGHEST
F32 = jnp.float32
BF16 = jnp.bfloat16
QUARTERS = 4
SLOTS = 4
GROUP = 4
CAP = 2
CHUNKS = 4
REACH = 4


def dot(a, b, dims=((1,), (0,)), precision=None):
    return lax.dot_general(a, b, (dims, ((), ())), preferred_element_type=F32, precision=precision)


def low(a, b, dims=((1,), (0,))):
    return dot(a.astype(BF16), b.astype(BF16), dims)


ROWS = ((0,), (0,))
LANES = ((1,), (1,))


def iota(shape, dim):
    return lax.broadcasted_iota(jnp.int32, shape, dim)


def sigmoid(x):
    return 1.0 / (1.0 + jnp.exp(-x))


def inverse(lower, row, col):
    eye = (row == col).astype(F32)
    near = jnp.where((row >> 3) == (col >> 3), lower, 0.0)
    second = dot(near, near, precision=HIGHEST)
    fourth = dot(second, second, precision=HIGHEST)
    found = dot(eye - near, eye + second, precision=HIGHEST)
    found = dot(found, eye + fourth, precision=HIGHEST)
    bit = 3
    while (1 << bit) < lower.shape[0]:
        across = ((row >> (bit + 1)) == (col >> (bit + 1))) & ((row >> bit) != (col >> bit))
        found = found - low(low(found, jnp.where(across, lower, 0.0)), found)
        bit += 1
    return found


def column_of(line, eye):
    return jnp.sum(jnp.where(eye, line, jnp.zeros_like(line)), axis=1, keepdims=True)


def line_of(column, eye):
    return jnp.sum(jnp.where(eye, column, jnp.zeros_like(column)), axis=0, keepdims=True)


def direction(reader, keys, values, unit, rates, log_decay, doc_col, doc_row, back):
    n = reader.shape[0]
    row, col = iota((n, n), 0), iota((n, n), 1)
    lane = iota((1, n), 1)
    first_head = lane < HEAD_DIM
    same_head = (row < HEAD_DIM) == (col < HEAD_DIM)
    upto = (col >= row) if back else (col <= row)
    match = doc_col == doc_row
    inclusive = upto & match
    strict = inclusive & (row != col)
    running = dot(upto.astype(F32), log_decay, precision=HIGHEST)
    total = running[:1] if back else running[n - 1 :]
    middle = 0.5 * total
    before = running - log_decay
    head_doc = doc_row[:, n - 1 :] if back else doc_row[:, :1]
    tail_doc = doc_row[:, :1] if back else doc_row[:, n - 1 :]
    opened = (doc_col == head_doc).astype(F32)
    closing = (doc_col == tail_doc).astype(F32)
    probe = unit * jnp.exp(before - middle)
    lifted = reader * jnp.exp(running - middle)
    undo = jnp.exp(middle - running)
    fix_keys = rates * unit * undo
    add_keys = keys * undo
    rest = jnp.exp(total - running)
    fix_last = rates * unit * rest
    add_last = keys * rest
    probe_open = opened * unit * jnp.exp(before)
    lifted_open = opened * reader * jnp.exp(running)
    left = jnp.concatenate([probe, lifted], axis=0)
    right = jnp.concatenate([fix_keys, add_keys], axis=0).astype(BF16)
    values_low = values.astype(BF16)
    removed, added, reads = [], [], []
    for head in range(2):
        mine = first_head if head == 0 else jnp.logical_not(first_head)
        grams = low(jnp.where(mine, left, 0.0), right, LANES)
        system = jnp.where(strict, grams[:n, :n], 0.0)
        add_mix = jnp.where(strict, grams[:n, n:], 0.0)
        reads.append(jnp.where(inclusive, grams[n:, :n], 0.0))
        read_add = jnp.where(inclusive, grams[n:, n:], 0.0)
        mixed = low(jnp.concatenate([add_mix, read_add], axis=0), values_low)
        added.append(mixed[n:])
        source = -jnp.concatenate([mixed[:n], probe_open], axis=1)
        removed.append(low(inverse(system, row, col), source))
    both = jnp.concatenate([first_head, first_head], axis=1)
    took = jnp.where(both, removed[0], removed[1])
    heads = [low(reads[head], took) for head in range(2)]
    through = jnp.where(both, heads[0], heads[1])
    outputs = through[:, :n] + jnp.where(first_head, added[0], added[1])
    response = through[:, n:] + lifted_open
    ends = low(took * closing, fix_last, ROWS)
    add = ends[:n] + low(values * closing, add_last, ROWS)
    whole = (head_doc == tail_doc).astype(F32)
    keep = ends[n:] + jnp.where(row == col, whole * jnp.exp(total), 0.0)
    add = jnp.where(same_head, add, 0.0)
    keep = jnp.where(same_head, keep, 0.0)
    half = n // 2
    element = jnp.concatenate(
        [
            keep[:half] + keep[half:],
            add[:half] + add[half:],
            jnp.broadcast_to(head_doc, (8, n)),
            jnp.broadcast_to(tail_doc, (8, n)),
        ],
        axis=0,
    ).astype(BF16)
    return outputs, response, element


def spread(block, same_head):
    return jnp.where(same_head, jnp.concatenate([block, block], axis=0), jnp.zeros_like(same_head, block.dtype))


def link(tail, head):
    return (tail == head).astype(F32)


def kernel(sizes, *refs):
    (
        receptance_ref, key_ref, value_ref, out_gate_ref, onward_ref, reverse_ref, rate_ref, extra_ref,
        docs_ref, head_scale_ref, mixer_hbm, residual_ref, expert_scale_ref, choice_ref, group_weight_ref,
        route_ref, gate_hbm, up_hbm, down_hbm,
        updated_ref,
        element, partner, chip, near, window, far, entering,
        mix_out, mixes, meta_out, meta_in, place, packed, arrived, pick, weigh_hi, weigh_lo,
        outward, inbound, answers, answered, combined, returned,
        mixer_w, gate_w, up_w, down_w,
        w_sem, pair_sem, near_send, near_recv, far_sem, mixer_send, mixer_recv, share_send, share_recv,
        mix_send, mix_recv, meta_send, meta_recv, out_send, out_recv, x_send, x_recv, y_send, y_recv,
        back_send, back_recv,
    ) = refs
    SP, TP = sizes
    chips = SP // 2
    sp, tp = lax.axis_index("sp"), lax.axis_index("tp")
    z, core = lax.div(sp, 2), lax.rem(sp, 2)
    n = receptance_ref.shape[0]
    count, width = residual_ref.shape
    quarter = width // QUARTERS
    piece = QUARTERS * SLOTS
    size = SP * piece
    group_slots = SP // CHUNKS
    chunk = group_slots * piece
    taken = group_slots * CAP

    barrier = pltpu.get_barrier_semaphore()

    def greet_sp(o, carry):
        pl.semaphore_signal(barrier, inc=1, device_id={"sp": lax.rem(sp + o, SP)}, device_id_type=MESH)
        return carry

    lax.fori_loop(1, SP, greet_sp, 0)
    for o in range(1, TP):
        pl.semaphore_signal(barrier, inc=1, device_id={"tp": lax.rem(tp + o, TP)}, device_id_type=MESH)

    loads = [
        pltpu.make_async_copy(src, dst, w_sem.at[k])
        for k, (src, dst) in enumerate(
            ((mixer_hbm, mixer_w.at[tp]), (gate_hbm, gate_w), (up_hbm, up_w), (down_hbm, down_w))
        )
    ]
    for load in loads:
        load.start()

    def turn(k):
        half = (k + 1) >> 1
        return SP // 2 + jnp.where((k & 1) == 1, -half, half)

    def ahead(k):
        peer = sp + turn(k)
        return jnp.where(peer >= SP, peer - SP, peer)

    def behind(k):
        peer = sp - turn(k)
        return jnp.where(peer < 0, peer + SP, peer)

    def sp_copy(src, dst, send, recv, k, back=False):
        return pltpu.make_async_remote_copy(
            src_ref=src, dst_ref=dst, send_sem=send.at[k], recv_sem=recv.at[k],
            device_id={"sp": behind(k) if back else ahead(k)}, device_id_type=MESH,
        )

    def rows_at(ref, k):
        return ref.at[pl.ds(pl.multiple_of(k * piece, piece), piece)]

    def meta_copy(k):
        return sp_copy(meta_out.at[k], meta_in.at[k], meta_send, meta_recv, k)

    def out_copy(k):
        return sp_copy(rows_at(packed, k), rows_at(arrived, k), out_send, out_recv, k)

    def home_copy(k):
        return sp_copy(rows_at(combined, k), rows_at(returned, k), back_send, back_recv, k, True)

    def each(make, act, first=0, last=SP - 1):
        def one(k, carry):
            act(make(k))
            return carry

        lax.fori_loop(first, last, one, 0)

    def begin(copy):
        copy.start()

    def leave(copy):
        copy.wait_send()

    def arrive(copy):
        copy.wait_recv()

    def bounds(c):
        return c * group_slots, min((c + 1) * group_slots, SP - 1)

    def tp_copy(src, dst, send, recv, k, o):
        return pltpu.make_async_remote_copy(
            src_ref=src, dst_ref=dst, send_sem=send.at[k], recv_sem=recv.at[k],
            device_id={"tp": lax.rem(tp + o, TP)}, device_id_type=MESH,
        )

    row, col = iota((n, n), 0), iota((n, n), 1)
    eye = row == col
    same_head = (row < HEAD_DIM) == (col < HEAD_DIM)
    first_head = iota((1, n), 1) < HEAD_DIM
    doc_row = docs_ref[...].astype(F32)
    doc_col = column_of(doc_row, eye)
    reader = receptance_ref[...].astype(F32)
    keys = key_ref[...].astype(F32)
    values = value_ref[...].astype(F32)

    def by_head(x):
        one = jnp.sum(jnp.where(first_head, x, 0.0), axis=1, keepdims=True)
        two = jnp.sum(jnp.where(first_head, 0.0, x), axis=1, keepdims=True)
        return jnp.where(first_head, one, two)

    unit = keys * lax.rsqrt(by_head(keys * keys) + 1e-06)
    rates = sigmoid(rate_ref[...].astype(F32))
    extra = jnp.where(first_head, column_of(extra_ref[:1], eye), column_of(extra_ref[1:2], eye))
    level = 0.6065306597126334
    onward = -level * sigmoid(onward_ref[...].astype(F32)) + extra
    reverse = -level * sigmoid(reverse_ref[...].astype(F32)) + extra
    out_f, resp_f, element_f = direction(reader, keys, values, unit, rates, onward, doc_col, doc_row, False)
    out_b, resp_b, element_b = direction(reader, keys, values, unit, rates, reverse, doc_col, doc_row, True)
    element[0] = element_f
    element[1] = element_b

    sign = 1 - 2 * core

    def pair_copy(src, dst, k):
        return pltpu.make_async_remote_copy(
            src_ref=src, dst_ref=dst, send_sem=pair_sem.at[2 * k], recv_sem=pair_sem.at[2 * k + 1],
            device_id={"sp": sp + sign}, device_id_type=MESH,
        )

    def chip_peer(distance):
        return lax.rem(z + sign * distance + chips, chips) * 2 + core

    def exists(distance):
        origin = z - sign * distance
        return (origin >= 0) & (origin < chips)

    half = n // 2

    def parts(ref_value):
        value = ref_value.astype(F32)
        return value[:half], value[half : 2 * half], value[n : n + 1], value[n + 8 : n + 9]

    pl.semaphore_wait(barrier, SP - 1 + TP - 1)
    first_copy = pair_copy(element.at[1 - core], partner, 0)
    first_copy.start()

    half_rows = n // 2
    own_rows = pl.ds(pl.multiple_of(core * half_rows, half_rows), half_rows)

    def block(o):
        return mixer_w.at[lax.rem(tp + o + TP, TP), own_rows]

    def round_copy(k):
        o, src = ((1, block(0)), (TP - 1, block(0)), (jnp.where(core == 0, 1, TP - 1), block(jnp.where(core == 0, -1, 1))))[k]
        return tp_copy(src, src, mixer_send, mixer_recv, k, o)

    def give_copy(o):
        src = block(o)
        return pltpu.make_async_remote_copy(
            src_ref=src, dst_ref=src, send_sem=share_send.at[o], recv_sem=share_recv.at[o],
            device_id={"sp": sp + sign}, device_id_type=MESH,
        )

    loads[0].wait()
    round_copy(0).start()
    round_copy(1).start()
    first_copy.wait()
    own = element[core].astype(F32)
    own_keep, own_add, own_head, own_tail = own[:half], own[half:n], own[n : n + 1], own[n + 8 : n + 9]
    par_keep, par_add, par_head, par_tail = parts(partner[...])
    joined = link(own_tail, par_head)
    both = joined * low(own[:n], spread(par_keep, same_head))
    chip[...] = jnp.concatenate(
        [both[:half], both[half:] + par_add, jnp.broadcast_to(own_head, (8, n)), jnp.broadcast_to(par_tail, (8, n))],
        axis=0,
    ).astype(BF16)

    def near_copy(k):
        return pltpu.make_async_remote_copy(
            src_ref=chip, dst_ref=near.at[k - 1], send_sem=near_send.at[k - 1], recv_sem=near_recv.at[k - 1],
            device_id={"sp": chip_peer(k)}, device_id_type=MESH,
        )

    for k in range(REACH, 0, -1):
        near_copy(k).start()

    lane32, row32 = iota((count, count), 1), iota((count, count), 0)
    eye32 = lane32 == row32
    choice = choice_ref[...].astype(F32)
    lead_line, trail_line = choice[:1], choice[1:2]
    lead, trail = column_of(lead_line, eye32), column_of(trail_line, eye32)
    lead_group = jnp.floor(lead * (1.0 / GROUP))
    group_line = line_of(lead_group, eye32)
    earlier = lane32 < row32

    def rank(mask):
        return jnp.sum(jnp.where(earlier & mask, 1.0, 0.0), axis=1, keepdims=True)

    slot = rank(lead_group == group_line)
    lead_rank = rank((lead == lead_line) | (lead == trail_line))
    trail_rank = rank((trail == lead_line) | (trail == trail_line))
    first_weight, second_weight = column_of(route_ref[:1], eye32), column_of(route_ref[1:2], eye32)
    scale = column_of(group_weight_ref[...], eye32) / (first_weight + second_weight)
    lane = iota((count, 128), 1).astype(F32)
    lead_own = lead - GROUP * lead_group + 2 * GROUP * slot
    trail_own = trail - GROUP * lead_group + 2 * GROUP * slot
    info = (
        jnp.where(lane == lead_own, lead_rank + 1.0, 0.0)
        + jnp.where(lane == trail_own, trail_rank + 1.0, 0.0)
        + jnp.where(lane == lead_own + GROUP, scale * first_weight, 0.0)
        + jnp.where(lane == trail_own + GROUP, scale * second_weight, 0.0)
    )
    goes = (ahead(iota((SP, count), 0)).astype(F32) == group_line).astype(F32)
    meta_out[...] = dot(goes, info, precision=HIGHEST).reshape(SP, 1, 128)
    each(meta_copy, begin)
    meta_in[SP - 1] = meta_out[SP - 1]
    stacked = QUARTERS * count
    group4, slot4 = jnp.concatenate([lead_group] * QUARTERS, 0), jnp.concatenate([slot] * QUARTERS, 0)
    at, at_row = iota((stacked, size), 1), iota((stacked, size), 0)
    table = (
        (group4 == ahead(at >> 4).astype(F32))
        & (slot4 == (at & 3).astype(F32))
        & (lax.div(at_row, count) == ((at >> 2) & 3))
    ).astype(F32)
    place[...] = table.T.astype(BF16)
    table = table.astype(BF16)
    round_copy(0).wait_recv()
    round_copy(1).wait_recv()
    round_copy(2).start()
    for k in range(1, REACH + 1):
        near_copy(k).wait_recv()
    keep, add, win_head, tail = parts(near[REACH - 1])
    tail = jnp.where(exists(REACH), tail, -1.0)
    for k in range(REACH - 1, 0, -1):
        next_keep, next_add, next_head, next_tail = parts(near[k - 1])
        step = link(tail, next_head) * low(
            jnp.concatenate([keep, add], axis=0), spread(next_keep, same_head)
        )
        keep, add = step[:half], step[half:] + next_add
        tail = jnp.where(exists(k), next_tail, -1.0)
    window[...] = jnp.concatenate(
        [add, jnp.broadcast_to(tail, (16, n))], axis=0
    ).astype(BF16)
    far_copy = pltpu.make_async_remote_copy(
        src_ref=window, dst_ref=far, send_sem=far_sem.at[0], recv_sem=far_sem.at[1],
        device_id={"sp": chip_peer(REACH)}, device_id_type=MESH,
    )
    far_copy.start()
    for k in range(1, REACH + 1):
        near_copy(k).wait_send()
    round_copy(2).wait_recv()
    for o in range(1, TP):
        give_copy(o).start()
    far_copy.wait()
    far_value = far[...].astype(F32)
    far_tail = jnp.where(exists(REACH), far_value[half : half + 1], -1.0)
    add = add + link(far_tail, win_head) * low(far_value[:half], spread(keep, same_head))
    state = link(tail, own_head) * add
    passed = (low(state, spread(own_keep, same_head)) + own_add) * joined
    entering[0] = passed.astype(BF16)
    last_copy = pair_copy(entering.at[0], entering.at[1], 1)
    last_copy.start()
    last_copy.wait()
    other = entering[1].astype(F32)
    state_f = jnp.where(core == 0, state, other)
    state_b = jnp.where(core == 0, other, state)
    entry = jnp.concatenate([spread(state_f, same_head), spread(state_b, same_head)], axis=1)
    mixed = out_f + out_b + low(jnp.concatenate([resp_f, resp_b], axis=1), entry, LANES)

    centred = mixed - by_head(mixed) * (1.0 / HEAD_DIM)
    scaled = centred * lax.rsqrt(by_head(centred * centred) * (1.0 / HEAD_DIM) + 0.00064)
    mix = (scaled * head_scale_ref[...] * sigmoid(out_gate_ref[...].astype(F32))).astype(BF16)
    for o in range(TP):
        mix_out[o] = mix[o * count : (o + 1) * count]

    def mix_copy(o):
        return tp_copy(mix_out.at[lax.rem(tp + o, TP)], mixes.at[tp], mix_send, mix_recv, o, o)

    for o in (2, 1, 3):
        mix_copy(o).start()
    mixes[tp] = mix_out[tp]
    for o in range(1, TP):
        give_copy(o).wait_recv()
    residual = residual_ref[...].astype(F32)
    for o in (1, 3, 2):
        mix_copy(o).wait_recv()
    wide = jnp.concatenate([mixes[o] for o in range(TP)], axis=1)
    hidden = residual + dot(wide, mixer_w[...].reshape(TP * n, width))
    hidden = hidden.astype(BF16).astype(F32)
    normed = (
        hidden * lax.rsqrt(jnp.mean(hidden * hidden, axis=1, keepdims=True) + 1e-06) * expert_scale_ref[...]
    ).astype(BF16)

    quarters = jnp.concatenate([normed[:, q * quarter : (q + 1) * quarter] for q in range(QUARTERS)], axis=0)
    packed[...] = dot(place[...], quarters).astype(BF16)
    each(out_copy, begin)
    arrived[size - piece :] = packed[size - piece :]

    each(meta_copy, arrive)
    told = meta_in[...].reshape(SP, 128)
    lane = iota((chunk, 128), 1)
    slot_lane = (iota((chunk, 128), 0) & 3) * (2 * GROUP)
    cols = QUARTERS * TP * taken
    row, col = iota((chunk, cols), 0), iota((chunk, cols), 1)
    col_q, col_o = lax.div(col, TP * taken), lax.rem(lax.div(col, taken), TP)
    col_k, col_e = lax.rem(lax.div(col, CAP), group_slots), (col & 1) + 1
    same_place = ((row >> 4) == col_k) & (((row >> 2) & 3) == col_q)
    source_row, source_col = iota((chunk, SP), 0), iota((chunk, SP), 1)
    for c in range(CHUNKS):
        widen = ((source_row >> 4) + c * group_slots == source_col).astype(F32)
        meta = dot(widen, told, precision=HIGHEST)
        codes, weights = jnp.zeros((chunk, cols), F32), jnp.zeros((chunk, cols), F32)
        for o in range(TP):
            at_code = slot_lane + lax.rem(tp + o, TP)
            code = jnp.sum(jnp.where(lane == at_code, meta, 0.0), axis=1, keepdims=True)
            weight = jnp.sum(jnp.where(lane == at_code + GROUP, meta, 0.0), axis=1, keepdims=True)
            codes, weights = jnp.where(col_o == o, code, codes), jnp.where(col_o == o, weight, weights)
        hit = same_place & (codes == col_e.astype(F32))
        pick[c] = jnp.where(hit, 1.0, 0.0).T.astype(BF16)
        weights = jnp.where(hit, weights, 0.0)
        high = weights.astype(BF16)
        weigh_hi[c] = high
        weigh_lo[c] = (weights - high.astype(F32)).astype(BF16)

    def to_expert(c, o):
        return tp_copy(outward.at[c, o], inbound.at[c, o], x_send, x_recv, c * TP + o, o)

    def from_expert(c, o):
        return tp_copy(answers.at[c, o], answered.at[c, o], y_send, y_recv, c * TP + o, TP - o)

    def take(c):
        each(out_copy, arrive, *bounds(c))
        rows = dot(pick[c], arrived[c * chunk : (c + 1) * chunk]).astype(BF16)
        for o in (2, 1, 3, 0):
            target = outward if o else inbound
            for q in range(QUARTERS):
                first = (q * TP + o) * taken
                target[c, o, :, q * quarter : (q + 1) * quarter] = rows[first : first + taken]
            if o:
                to_expert(c, o).start()

    def work(c):
        for o in (1, 3, 2):
            to_expert(c, o).wait_recv()
        rows = inbound[c].reshape(TP * taken, width)
        gate = dot(rows, gate_w[...])
        up = dot(rows, up_w[...])
        active = (gate * sigmoid(gate) * up).astype(BF16)
        result = dot(active, down_w[...]).astype(BF16)
        for o in (2, 1, 3, 0):
            target = answers if o else answered
            target[c, o] = result[o * taken : (o + 1) * taken]
            if o:
                from_expert(c, o).start()

    def give(c):
        for o in (1, 3, 2):
            from_expert(c, o).wait_recv()
        flat = answered[c].reshape(TP * taken, width)
        flat = jnp.concatenate([flat[:, q * quarter : (q + 1) * quarter] for q in range(QUARTERS)], axis=0)
        at = slice(c * chunk, (c + 1) * chunk)
        combined[at] = (dot(weigh_hi[c], flat) + dot(weigh_lo[c], flat)).astype(BF16)
        each(home_copy, begin, *bounds(c))

    for load in loads[1:]:
        load.wait()
    take(0)
    work(0)
    take(1)
    give(0)
    take(2)
    take(3)
    work(1)
    work(2)
    give(1)
    work(3)
    give(2)
    give(3)
    returned[size - piece :] = combined[size - piece :]

    for k in range(3):
        round_copy(k).wait_send()
    for o in range(1, TP):
        give_copy(o).wait_send()
        mix_copy(o).wait_send()
        for c in range(CHUNKS):
            to_expert(c, o).wait_send()
            from_expert(c, o).wait_send()
    each(meta_copy, leave)
    each(out_copy, leave)
    final = jnp.zeros((stacked, quarter), F32)
    for c in range(CHUNKS):
        each(home_copy, arrive, *bounds(c))
        at = slice(c * chunk, (c + 1) * chunk)
        final += dot(table[:, at], returned[at])
    for q in range(QUARTERS):
        at = slice(q * quarter, (q + 1) * quarter)
        updated_ref[:, at] = (hidden[:, at] + final[q * count : (q + 1) * count]).astype(BF16)

    each(home_copy, leave)


def solution(mesh):
    SP, TP = mesh.shape["sp"], mesh.shape["tp"]

    def body(
        receptance, key_matrix, value_matrix, output_gate_logits, onward_decay_logits, reverse_decay_logits,
        correction_rate_logits, extra_log_decay, documents, head_norm_scale, mixer_output_weight, residual,
        expert_norm_scale, expert_choice_index, group_route_weight, expert_route_weight,
        expert_gate_matrix, expert_up_matrix, expert_down_matrix,
    ):
        n, channels = receptance.shape
        count, width = residual.shape
        hidden_units = expert_gate_matrix.shape[2]
        piece = QUARTERS * SLOTS
        size, quarter = SP * piece, width // QUARTERS
        chunk, taken = size // CHUNKS, SP // CHUNKS * CAP
        vmem, hbm = pl.BlockSpec(memory_space=pltpu.VMEM), pl.BlockSpec(memory_space=pl.ANY)
        dma = pltpu.SemaphoreType.DMA
        return pl.pallas_call(
            functools.partial(kernel, (SP, TP)),
            out_shape=jax.ShapeDtypeStruct((count, width), BF16),
            in_specs=[vmem] * 10 + [hbm] + [vmem] * 5 + [hbm] * 3,
            out_specs=vmem,
            scratch_shapes=[
                pltpu.VMEM((2, n + 16, n), BF16),
                pltpu.VMEM((n + 16, n), BF16),
                pltpu.VMEM((n + 16, n), BF16),
                pltpu.VMEM((REACH, n + 16, n), BF16),
                pltpu.VMEM((n // 2 + 16, n), BF16),
                pltpu.VMEM((n // 2 + 16, n), BF16),
                pltpu.VMEM((2, n // 2, n), BF16),
                pltpu.VMEM((TP, count, channels), BF16),
                pltpu.VMEM((TP, count, channels), BF16),
                pltpu.VMEM((SP, 1, 128), F32),
                pltpu.VMEM((SP, 1, 128), F32),
                pltpu.VMEM((size, QUARTERS * count), BF16),
                pltpu.VMEM((size, quarter), BF16),
                pltpu.VMEM((size, quarter), BF16),
                pltpu.VMEM((CHUNKS, QUARTERS * TP * taken, chunk), BF16),
                pltpu.VMEM((CHUNKS, chunk, QUARTERS * TP * taken), BF16),
                pltpu.VMEM((CHUNKS, chunk, QUARTERS * TP * taken), BF16),
                pltpu.VMEM((CHUNKS, TP, taken, width), BF16),
                pltpu.VMEM((CHUNKS, TP, taken, width), BF16),
                pltpu.VMEM((CHUNKS, TP, taken, width), BF16),
                pltpu.VMEM((CHUNKS, TP, taken, width), BF16),
                pltpu.VMEM((size, quarter), BF16),
                pltpu.VMEM((size, quarter), BF16),
                pltpu.VMEM((TP, channels, width), BF16),
                pltpu.VMEM((width, hidden_units), BF16),
                pltpu.VMEM((width, hidden_units), BF16),
                pltpu.VMEM((hidden_units, width), BF16),
                dma((4,)), dma((4,)), dma((REACH,)), dma((REACH,)), dma((2,)), dma((3,)), dma((3,)),
                dma((TP,)), dma((TP,)), dma((TP,)), dma((TP,)), dma((SP,)), dma((SP,)), dma((SP,)), dma((SP,)),
                dma((CHUNKS * TP,)), dma((CHUNKS * TP,)), dma((CHUNKS * TP,)), dma((CHUNKS * TP,)),
                dma((SP,)), dma((SP,)),
            ],
            compiler_params=pltpu.CompilerParams(
                collective_id=0, has_side_effects=True, vmem_limit_bytes=56 * 1024 * 1024
            ),
        )(
            receptance, key_matrix, value_matrix, output_gate_logits, onward_decay_logits, reverse_decay_logits,
            correction_rate_logits, extra_log_decay.T, documents.reshape(1, n), head_norm_scale.reshape(1, channels),
            mixer_output_weight, residual, expert_norm_scale.reshape(1, width), expert_choice_index.T,
            group_route_weight.reshape(1, count), expert_route_weight.T,
            expert_gate_matrix[0], expert_up_matrix[0], expert_down_matrix[0],
        )

    in_specs = (
        (P(GRP_SP, "tp"),) * 8
        + (P(GRP_SP), P("tp"), P("tp", None), P(GRP_SP_TP, None), P(), P(GRP_SP_TP, None))
        + (P(GRP_SP_TP), P(GRP_SP_TP, None))
        + (P(SP_TP, None, None),) * 3
    )
    return jax.shard_map(
        body, mesh=mesh, in_specs=in_specs, out_specs=P(GRP_SP_TP, None), check_vma=False
    )
```

```python
import functools

import jax
import jax.numpy as jnp
from jax import lax
from jax.experimental import pallas as pl
from jax.experimental.pallas import tpu as pltpu
from jax.sharding import PartitionSpec as P

HEAD_DIM = 64
GRP_SP = ("grp", "sp")
GRP_SP_TP = ("grp", "sp", "tp")
SP_TP = ("sp", "tp")
MESH = pl.DeviceIdType.MESH
HIGHEST = lax.Precision.HIGHEST
F32 = jnp.float32
BF16 = jnp.bfloat16
QUARTERS = 4
SLOTS = 4
GROUP = 4
CAP = 2
CHUNKS = 4
REACH = 4


def dot(a, b, dims=((1,), (0,)), precision=None):
    return lax.dot_general(a, b, (dims, ((), ())), preferred_element_type=F32, precision=precision)


def low(a, b, dims=((1,), (0,))):
    return dot(a.astype(BF16), b.astype(BF16), dims)


ROWS = ((0,), (0,))
LANES = ((1,), (1,))


def iota(shape, dim):
    return lax.broadcasted_iota(jnp.int32, shape, dim)


def sigmoid(x):
    return 1.0 / (1.0 + jnp.exp(-x))


def inverse(lower, row, col):
    eye = (row == col).astype(F32)
    near = jnp.where((row >> 3) == (col >> 3), lower, 0.0)
    second = dot(near, near, precision=HIGHEST)
    fourth = dot(second, second, precision=HIGHEST)
    found = dot(eye - near, eye + second, precision=HIGHEST)
    found = dot(found, eye + fourth, precision=HIGHEST)
    bit = 3
    while (1 << bit) < lower.shape[0]:
        across = ((row >> (bit + 1)) == (col >> (bit + 1))) & ((row >> bit) != (col >> bit))
        found = found - low(low(found, jnp.where(across, lower, 0.0)), found)
        bit += 1
    return found


def column_of(line, eye):
    return jnp.sum(jnp.where(eye, line, jnp.zeros_like(line)), axis=1, keepdims=True)


def line_of(column, eye):
    return jnp.sum(jnp.where(eye, column, jnp.zeros_like(column)), axis=0, keepdims=True)


def direction(reader, keys, values, unit, rates, log_decay, doc_col, doc_row, back):
    n = reader.shape[0]
    row, col = iota((n, n), 0), iota((n, n), 1)
    lane = iota((1, n), 1)
    first_head = lane < HEAD_DIM
    same_head = (row < HEAD_DIM) == (col < HEAD_DIM)
    upto = (col >= row) if back else (col <= row)
    match = doc_col == doc_row
    inclusive = upto & match
    strict = inclusive & (row != col)
    running = dot(upto.astype(F32), log_decay, precision=HIGHEST)
    total = running[:1] if back else running[n - 1 :]
    middle = 0.5 * total
    before = running - log_decay
    head_doc = doc_row[:, n - 1 :] if back else doc_row[:, :1]
    tail_doc = doc_row[:, :1] if back else doc_row[:, n - 1 :]
    opened = (doc_col == head_doc).astype(F32)
    closing = (doc_col == tail_doc).astype(F32)
    probe = unit * jnp.exp(before - middle)
    lifted = reader * jnp.exp(running - middle)
    undo = jnp.exp(middle - running)
    fix_keys = rates * unit * undo
    add_keys = keys * undo
    rest = jnp.exp(total - running)
    fix_last = rates * unit * rest
    add_last = keys * rest
    probe_open = opened * unit * jnp.exp(before)
    lifted_open = opened * reader * jnp.exp(running)
    left = jnp.concatenate([probe, lifted], axis=0)
    right = jnp.concatenate([fix_keys, add_keys], axis=0).astype(BF16)
    values_low = values.astype(BF16)
    added, reads, inverses, sources = [], [], [], []
    for head in range(2):
        mine = first_head if head == 0 else jnp.logical_not(first_head)
        grams = low(jnp.where(mine, left, 0.0), right, LANES)
        system = jnp.where(strict, grams[:n, :n], 0.0)
        add_mix = jnp.where(strict, grams[:n, n:], 0.0)
        reads.append(jnp.where(inclusive, grams[n:, :n], 0.0))
        read_add = jnp.where(inclusive, grams[n:, n:], 0.0)
        mixed = low(jnp.concatenate([add_mix, read_add], axis=0), values_low)
        added.append(mixed[n:])
        sources.append(-jnp.concatenate([mixed[:n], probe_open], axis=1))
        inverses.append(inverse(system, row, col))
    yield None
    removed = [low(inverses[head], sources[head]) for head in range(2)]
    both = jnp.concatenate([first_head, first_head], axis=1)
    took = jnp.where(both, removed[0], removed[1])
    heads = [low(reads[head], took) for head in range(2)]
    through = jnp.where(both, heads[0], heads[1])
    outputs = through[:, :n] + jnp.where(first_head, added[0], added[1])
    response = through[:, n:] + lifted_open
    ends = low(took * closing, fix_last, ROWS)
    add = ends[:n] + low(values * closing, add_last, ROWS)
    whole = (head_doc == tail_doc).astype(F32)
    keep = ends[n:] + jnp.where(row == col, whole * jnp.exp(total), 0.0)
    add = jnp.where(same_head, add, 0.0)
    keep = jnp.where(same_head, keep, 0.0)
    half = n // 2
    element = jnp.concatenate(
        [
            keep[:half] + keep[half:],
            add[:half] + add[half:],
            jnp.broadcast_to(head_doc, (8, n)),
            jnp.broadcast_to(tail_doc, (8, n)),
        ],
        axis=0,
    ).astype(BF16)
    yield outputs, response, element


def spread(block, same_head):
    return jnp.where(same_head, jnp.concatenate([block, block], axis=0), jnp.zeros_like(same_head, block.dtype))


def link(tail, head):
    return (tail == head).astype(F32)


def kernel(sizes, *refs):
    (
        receptance_ref, key_ref, value_ref, out_gate_ref, onward_ref, reverse_ref, rate_ref, extra_ref,
        docs_ref, head_scale_ref, mixer_hbm, residual_ref, expert_scale_ref, choice_ref, group_weight_ref,
        route_ref, gate_hbm, up_hbm, down_hbm,
        updated_ref,
        element, partner, chip, came, far, entering,
        mix_out, mixes, meta_out, meta_in, place, packed, arrived, packed_mix, arrived_mix, pick, weigh_hi, weigh_lo,
        outward, inbound, outward_mix, inbound_mix, answers, answered, combined, returned,
        mixer_w, gate_w, up_w, down_w,
        w_sem, pair_sem, scan_send, scan_recv, mixer_send, mixer_recv, share_send, share_recv,
        mix_send, mix_recv, meta_send, meta_recv, out_send, out_recv, late_send, late_recv, x_send, x_recv,
        m_send, m_recv, y_send, y_recv,        back_send, back_recv,
    ) = refs
    SP, TP = sizes
    chips = SP // 2
    sp, tp = lax.axis_index("sp"), lax.axis_index("tp")
    z, core = lax.div(sp, 2), lax.rem(sp, 2)
    n = receptance_ref.shape[0]
    count, width = residual_ref.shape
    quarter = width // QUARTERS
    piece = QUARTERS * SLOTS
    size = SP * piece
    group_slots = SP // CHUNKS
    chunk = group_slots * piece
    taken = group_slots * CAP

    barrier = pltpu.get_barrier_semaphore()

    def greet_sp(o, carry):
        pl.semaphore_signal(barrier, inc=1, device_id={"sp": lax.rem(sp + o, SP)}, device_id_type=MESH)
        return carry

    lax.fori_loop(1, SP, greet_sp, 0)
    for o in range(1, TP):
        pl.semaphore_signal(barrier, inc=1, device_id={"tp": lax.rem(tp + o, TP)}, device_id_type=MESH)

    loads = [
        pltpu.make_async_copy(src, dst, w_sem.at[k])
        for k, (src, dst) in enumerate(
            ((mixer_hbm, mixer_w.at[tp]), (gate_hbm, gate_w), (up_hbm, up_w), (down_hbm, down_w))
        )
    ]
    for load in loads:
        load.start()

    def turn(k):
        half = (k + 1) >> 1
        if isinstance(k, int):
            return SP // 2 + (-half if k & 1 else half)
        return SP // 2 + jnp.where((k & 1) == 1, -half, half)

    def ahead(k):
        peer = sp + turn(k)
        return jnp.where(peer >= SP, peer - SP, peer)

    def behind(k):
        peer = sp - turn(k)
        return jnp.where(peer < 0, peer + SP, peer)

    def sp_copy(src, dst, send, recv, k, back=False):
        return pltpu.make_async_remote_copy(
            src_ref=src, dst_ref=dst, send_sem=send.at[k], recv_sem=recv.at[k],
            device_id={"sp": behind(k) if back else ahead(k)}, device_id_type=MESH,
        )

    def rows_at(ref, k):
        return ref.at[pl.ds(pl.multiple_of(k * piece, piece), piece)]

    def meta_copy(k):
        return sp_copy(meta_out.at[k], meta_in.at[k], meta_send, meta_recv, k)

    def out_copy(k):
        return sp_copy(rows_at(packed, k), rows_at(arrived, k), out_send, out_recv, k)

    def late_copy(k):
        return sp_copy(rows_at(packed_mix, k), rows_at(arrived_mix, k), late_send, late_recv, k)

    def home_copy(k):
        return sp_copy(rows_at(combined, k), rows_at(returned, k), back_send, back_recv, k, True)

    def begin(copy):
        copy.start()

    def each(make, act, first=0, last=SP - 1):
        if act is begin:
            for k in range(first, last):
                act(make(k))
            return

        def one(k, carry):
            act(make(k))
            return carry

        lax.fori_loop(first, last, one, 0)

    def leave(copy):
        copy.wait_send()

    def arrive(copy):
        copy.wait_recv()

    def bounds(c):
        return c * group_slots, min((c + 1) * group_slots, SP - 1)

    def tp_copy(src, dst, send, recv, k, o):
        return pltpu.make_async_remote_copy(
            src_ref=src, dst_ref=dst, send_sem=send.at[k], recv_sem=recv.at[k],
            device_id={"tp": lax.rem(tp + o, TP)}, device_id_type=MESH,
        )

    lane32, row32 = iota((count, count), 1), iota((count, count), 0)
    eye32 = lane32 == row32
    choice = choice_ref[...].astype(F32)
    lead_line, trail_line = choice[:1], choice[1:2]
    lead, trail = column_of(lead_line, eye32), column_of(trail_line, eye32)
    lead_group = jnp.floor(lead * (1.0 / GROUP))
    group_line = line_of(lead_group, eye32)
    earlier = lane32 < row32

    def rank(mask):
        return jnp.sum(jnp.where(earlier & mask, 1.0, 0.0), axis=1, keepdims=True)

    slot = rank(lead_group == group_line)
    lead_rank = rank((lead == lead_line) | (lead == trail_line))
    trail_rank = rank((trail == lead_line) | (trail == trail_line))
    first_weight, second_weight = column_of(route_ref[:1], eye32), column_of(route_ref[1:2], eye32)
    scale = column_of(group_weight_ref[...], eye32) / (first_weight + second_weight)
    lane = iota((count, 128), 1).astype(F32)
    lead_own = lead - GROUP * lead_group + 2 * GROUP * slot
    trail_own = trail - GROUP * lead_group + 2 * GROUP * slot
    info = (
        jnp.where(lane == lead_own, lead_rank + 1.0, 0.0)
        + jnp.where(lane == trail_own, trail_rank + 1.0, 0.0)
        + jnp.where(lane == lead_own + GROUP, scale * first_weight, 0.0)
        + jnp.where(lane == trail_own + GROUP, scale * second_weight, 0.0)
    )
    goes = (ahead(iota((SP, count), 0)).astype(F32) == group_line).astype(F32)
    meta_out[...] = dot(goes, info, precision=HIGHEST).reshape(SP, 1, 128)
    stacked = QUARTERS * count
    group4, slot4 = jnp.concatenate([lead_group] * QUARTERS, 0), jnp.concatenate([slot] * QUARTERS, 0)
    at, at_row = iota((stacked, size), 1), iota((stacked, size), 0)
    table = (
        (group4 == ahead(at >> 4).astype(F32))
        & (slot4 == (at & 3).astype(F32))
        & (lax.div(at_row, count) == ((at >> 2) & 3))
    ).astype(F32)
    place[...] = table.T.astype(BF16)
    table = table.astype(BF16)

    def by_quarter(rows):
        part = rows.shape[1] // QUARTERS
        return jnp.concatenate([rows[:, q * part : (q + 1) * part] for q in range(QUARTERS)], axis=0)

    packed[...] = dot(place[...], by_quarter(residual_ref[...])).astype(BF16)

    row, col = iota((n, n), 0), iota((n, n), 1)
    eye = row == col
    same_head = (row < HEAD_DIM) == (col < HEAD_DIM)
    first_head = iota((1, n), 1) < HEAD_DIM
    doc_row = docs_ref[...].astype(F32)
    doc_col = column_of(doc_row, eye)
    reader = receptance_ref[...].astype(F32)
    keys = key_ref[...].astype(F32)
    values = value_ref[...].astype(F32)

    def by_head(x):
        one = jnp.sum(jnp.where(first_head, x, 0.0), axis=1, keepdims=True)
        two = jnp.sum(jnp.where(first_head, 0.0, x), axis=1, keepdims=True)
        return jnp.where(first_head, one, two)

    unit = keys * lax.rsqrt(by_head(keys * keys) + 1e-06)
    rates = sigmoid(rate_ref[...].astype(F32))
    extra = jnp.where(first_head, column_of(extra_ref[:1], eye), column_of(extra_ref[1:2], eye))
    level = 0.6065306597126334
    onward = -level * sigmoid(onward_ref[...].astype(F32)) + extra
    reverse = -level * sigmoid(reverse_ref[...].astype(F32)) + extra
    forward = direction(reader, keys, values, unit, rates, onward, doc_col, doc_row, False)
    backward = direction(reader, keys, values, unit, rates, reverse, doc_col, doc_row, True)
    next(forward)
    next(backward)

    pl.semaphore_wait(barrier, SP - 1 + TP - 1)

    out_f, resp_f, element_f = next(forward)
    out_b, resp_b, element_b = next(backward)
    element[0] = element_f
    element[1] = element_b

    sign = 1 - 2 * core

    def pair_copy(src, dst, k):
        return pltpu.make_async_remote_copy(
            src_ref=src, dst_ref=dst, send_sem=pair_sem.at[2 * k], recv_sem=pair_sem.at[2 * k + 1],
            device_id={"sp": sp + sign}, device_id_type=MESH,
        )

    def chip_peer(distance):
        return lax.rem(z + sign * distance + chips, chips) * 2 + core

    def exists(distance):
        origin = z - sign * distance
        return (origin >= 0) & (origin < chips)

    half = n // 2

    def parts(ref_value):
        value = ref_value.astype(F32)
        return value[:half], value[half : 2 * half], value[n : n + 1], value[n + 8 : n + 9]

    first_copy = pair_copy(element.at[1 - core], partner, 0)
    first_copy.start()

    half_rows = n // 2
    own_rows = pl.ds(pl.multiple_of(core * half_rows, half_rows), half_rows)

    def block(o):
        return mixer_w.at[lax.rem(tp + o + TP, TP), own_rows]

    def round_copy(k):
        o, src = ((1, block(0)), (TP - 1, block(0)), (jnp.where(core == 0, 1, TP - 1), block(jnp.where(core == 0, -1, 1))))[k]
        return tp_copy(src, src, mixer_send, mixer_recv, k, o)

    def give_copy(o):
        src = block(o)
        return pltpu.make_async_remote_copy(
            src_ref=src, dst_ref=src, send_sem=share_send.at[o], recv_sem=share_recv.at[o],
            device_id={"sp": sp + sign}, device_id_type=MESH,
        )

    loads[0].wait()
    round_copy(0).start()
    round_copy(1).start()
    each(meta_copy, begin)
    meta_in[SP - 1] = meta_out[SP - 1]
    each(out_copy, begin, *bounds(3))
    arrived[size - piece :] = packed[size - piece :]
    first_copy.wait()
    own = element[core].astype(F32)
    own_keep, own_add, own_head, own_tail = own[:half], own[half:n], own[n : n + 1], own[n + 8 : n + 9]
    par_keep, par_add, par_head, par_tail = parts(partner[...])
    joined = link(own_tail, par_head)
    both = joined * low(own[:n], spread(par_keep, same_head))
    def keep_element(at, both, head, tail):
        chip[at] = jnp.concatenate(
            [both, jnp.broadcast_to(head, (8, n)), jnp.broadcast_to(tail, (8, n))], axis=0
        ).astype(BF16)

    zeros = jnp.zeros((half, n), F32)
    window = both + jnp.concatenate([zeros, par_add], axis=0)
    head, tail = own_head, par_tail

    def scan_copy(k):
        src, dst, distance = (
            (chip.at[0], came.at[0], 1),
            (chip.at[1], came.at[1], 2),
            (chip.at[2], came.at[2], 1),
            (far.at[0], far.at[1], REACH + 1),
        )[k]
        return pltpu.make_async_remote_copy(
            src_ref=src, dst_ref=dst, send_sem=scan_send.at[k], recv_sem=scan_recv.at[k],
            device_id={"sp": chip_peer(distance)}, device_id_type=MESH,
        )

    def doubled(k, distance, window, head):
        past_keep, past_add, past_head, past_tail = parts(came[k])
        past_tail = jnp.where(exists(distance), past_tail, -1.0)
        joined = link(past_tail, head) * low(
            jnp.concatenate([past_keep, past_add], axis=0), spread(window[:half], same_head)
        )
        return joined + jnp.concatenate([zeros, window[half:]], axis=0), past_head

    keep_element(0, window, head, tail)
    scan_copy(0).start()
    scan_copy(0).wait_recv()
    window, head = doubled(0, 1, window, head)
    keep_element(1, window, head, tail)
    scan_copy(1).start()
    round_copy(0).wait_recv()
    round_copy(1).wait_recv()
    round_copy(2).start()
    scan_copy(1).wait_recv()
    window, head = doubled(1, 2, window, head)
    far[0] = jnp.concatenate([window[half:], jnp.broadcast_to(tail, (16, n))], axis=0).astype(BF16)
    scan_copy(3).start()
    keep_element(2, window, head, tail)
    scan_copy(2).start()
    each(out_copy, begin, *bounds(2))

    each(meta_copy, arrive)
    told = meta_in[...].reshape(SP, 128)
    lane = iota((chunk, 128), 1)
    slot_lane = (iota((chunk, 128), 0) & 3) * (2 * GROUP)
    cols = QUARTERS * TP * taken
    row, col = iota((chunk, cols), 0), iota((chunk, cols), 1)
    col_q, col_o = lax.div(col, TP * taken), lax.rem(lax.div(col, taken), TP)
    col_k, col_e = lax.rem(lax.div(col, CAP), group_slots), (col & 1) + 1
    same_place = ((row >> 4) == col_k) & (((row >> 2) & 3) == col_q)
    source_row, source_col = iota((chunk, SP), 0), iota((chunk, SP), 1)
    for c in range(CHUNKS):
        widen = ((source_row >> 4) + c * group_slots == source_col).astype(F32)
        meta = dot(widen, told, precision=HIGHEST)
        codes, weights = jnp.zeros((chunk, cols), F32), jnp.zeros((chunk, cols), F32)
        for o in range(TP):
            at_code = slot_lane + lax.rem(tp + o, TP)
            code = jnp.sum(jnp.where(lane == at_code, meta, 0.0), axis=1, keepdims=True)
            weight = jnp.sum(jnp.where(lane == at_code + GROUP, meta, 0.0), axis=1, keepdims=True)
            codes, weights = jnp.where(col_o == o, code, codes), jnp.where(col_o == o, weight, weights)
        hit = same_place & (codes == col_e.astype(F32))
        pick[c] = jnp.where(hit, 1.0, 0.0).T.astype(BF16)
        weights = jnp.where(hit, weights, 0.0)
        high = weights.astype(BF16)
        weigh_hi[c] = high
        weigh_lo[c] = (weights - high.astype(F32)).astype(BF16)

    round_copy(2).wait_recv()
    for o in range(1, TP):
        give_copy(o).start()
    scan_copy(2).wait_recv()
    keep, add, past_head, past_tail = parts(came[2])
    keep = spread(keep, same_head)
    scan_copy(3).wait_recv()
    far_value = far[1].astype(F32)
    far_tail = jnp.where(exists(REACH + 1), far_value[half : half + 1], -1.0)
    add = add + link(far_tail, past_head) * low(far_value[:half], keep)
    tail = jnp.where(exists(1), past_tail, -1.0)
    state = link(tail, own_head) * add
    passed = (low(state, spread(own_keep, same_head)) + own_add) * joined
    entering[0] = passed.astype(BF16)
    last_copy = pair_copy(entering.at[0], entering.at[1], 1)
    last_copy.start()
    each(out_copy, begin, *bounds(0))
    last_copy.wait()
    other = entering[1].astype(F32)
    state_f = jnp.where(core == 0, state, other)
    state_b = jnp.where(core == 0, other, state)
    entry = jnp.concatenate([spread(state_f, same_head), spread(state_b, same_head)], axis=1)
    mixed = out_f + out_b + low(jnp.concatenate([resp_f, resp_b], axis=1), entry, LANES)

    centred = mixed - by_head(mixed) * (1.0 / HEAD_DIM)
    scaled = centred * lax.rsqrt(by_head(centred * centred) * (1.0 / HEAD_DIM) + 0.00064)
    mix = (scaled * head_scale_ref[...] * sigmoid(out_gate_ref[...].astype(F32))).astype(BF16)
    for o in range(TP):
        mix_out[o] = mix[o * count : (o + 1) * count]

    def mix_copy(o):
        return tp_copy(mix_out.at[lax.rem(tp + o, TP)], mixes.at[tp], mix_send, mix_recv, o, o)

    for o in (2, 1, 3):
        mix_copy(o).start()
    mixes[tp] = mix_out[tp]
    for o in (1, 3, 2):
        mix_copy(o).wait_recv()
    packed_mix[...] = dot(place[...], mixes[...].reshape(TP * count, n)).astype(BF16)
    each(late_copy, begin, *bounds(2))
    each(late_copy, begin, *bounds(0))
    each(late_copy, begin, *bounds(1))
    each(late_copy, begin, *bounds(3))
    each(out_copy, begin, *bounds(1))
    arrived_mix[size - piece :] = packed_mix[size - piece :]

    def to_expert(c, o):
        return tp_copy(outward.at[c, o], inbound.at[c, o], x_send, x_recv, c * TP + o, o)

    def to_expert_mix(c, o):
        return tp_copy(outward_mix.at[c, o], inbound_mix.at[c, o], m_send, m_recv, c * TP + o, o)

    def from_expert(c, o):
        return tp_copy(answers.at[c, o], answered.at[c, o], y_send, y_recv, c * TP + o, TP - o)

    def take(c, copy, source, theirs, ours, send):
        each(copy, arrive, *bounds(c))
        rows = dot(pick[c], source[c * chunk : (c + 1) * chunk]).astype(BF16)
        part = rows.shape[1]
        for o in (2, 1, 3, 0):
            target = theirs if o else ours
            for q in range(QUARTERS):
                first = (q * TP + o) * taken
                target[c, o, :, q * part : (q + 1) * part] = rows[first : first + taken]
            if o:
                send(c, o).start()

    def norm(rows):
        rows = rows * lax.rsqrt(jnp.mean(rows * rows, axis=1, keepdims=True) + 1e-06)
        return (rows * expert_scale_ref[...]).astype(BF16)

    def project(rows, channels):
        rows = rows.astype(F32) + dot(channels, mixer_w[...].reshape(TP * n, width))
        return rows.astype(BF16).astype(F32)

    def work(c):
        for o in (1, 3, 2):
            to_expert(c, o).wait_recv()
        for o in (1, 3, 2):
            to_expert_mix(c, o).wait_recv()
        rows = inbound[c].reshape(TP * taken, width)
        rows = norm(project(rows, inbound_mix[c].reshape(TP * taken, TP * n)))
        gate = dot(rows, gate_w[...])
        up = dot(rows, up_w[...])
        active = (gate * sigmoid(gate) * up).astype(BF16)
        result = dot(active, down_w[...]).astype(BF16)
        for o in (2, 1, 3, 0):
            target = answers if o else answered
            target[c, o] = result[o * taken : (o + 1) * taken]
            if o:
                from_expert(c, o).start()

    def give(c):
        for o in (1, 3, 2):
            from_expert(c, o).wait_recv()
        flat = answered[c].reshape(TP * taken, width)
        flat = by_quarter(flat)
        at = slice(c * chunk, (c + 1) * chunk)
        combined[at] = (dot(weigh_hi[c], flat) + dot(weigh_lo[c], flat)).astype(BF16)
        each(home_copy, begin, *bounds(c))

    for load in loads[1:]:
        load.wait()
    def take_early(c):
        take(c, out_copy, arrived, outward, inbound, to_expert)

    def take_late(c):
        take(c, late_copy, arrived_mix, outward_mix, inbound_mix, to_expert_mix)

    take_early(3)
    take_early(2)
    take_early(0)
    for o in range(1, TP):
        give_copy(o).wait_recv()
    hidden = project(residual_ref[...], jnp.concatenate([mixes[o] for o in range(TP)], axis=1))
    take_late(2)
    take_late(0)
    take_late(3)
    take_late(1)
    work(2)
    take_early(1)
    work(0)
    work(3)
    give(2)
    give(0)
    work(1)
    give(3)
    give(1)
    returned[size - piece :] = combined[size - piece :]

    for k in range(3):
        round_copy(k).wait_send()
    for k in range(4):
        scan_copy(k).wait_send()
    for o in range(1, TP):
        give_copy(o).wait_send()
        mix_copy(o).wait_send()
        for c in range(CHUNKS):
            to_expert(c, o).wait_send()
            to_expert_mix(c, o).wait_send()
            from_expert(c, o).wait_send()
    each(meta_copy, leave)
    each(out_copy, leave)
    each(late_copy, leave)
    final = jnp.zeros((stacked, quarter), F32)
    for c in range(CHUNKS):
        each(home_copy, arrive, *bounds(c))
        at = slice(c * chunk, (c + 1) * chunk)
        final += dot(table[:, at], returned[at])
    for q in range(QUARTERS):
        at = slice(q * quarter, (q + 1) * quarter)
        updated_ref[:, at] = (hidden[:, at] + final[q * count : (q + 1) * count]).astype(BF16)

    each(home_copy, leave)


def solution(mesh):
    SP, TP = mesh.shape["sp"], mesh.shape["tp"]

    def body(
        receptance, key_matrix, value_matrix, output_gate_logits, onward_decay_logits, reverse_decay_logits,
        correction_rate_logits, extra_log_decay, documents, head_norm_scale, mixer_output_weight, residual,
        expert_norm_scale, expert_choice_index, group_route_weight, expert_route_weight,
        expert_gate_matrix, expert_up_matrix, expert_down_matrix,
    ):
        n, channels = receptance.shape
        count, width = residual.shape
        hidden_units = expert_gate_matrix.shape[2]
        piece = QUARTERS * SLOTS
        size, quarter = SP * piece, width // QUARTERS
        chunk, taken = size // CHUNKS, SP // CHUNKS * CAP
        vmem, hbm = pl.BlockSpec(memory_space=pltpu.VMEM), pl.BlockSpec(memory_space=pl.ANY)
        dma = pltpu.SemaphoreType.DMA
        return pl.pallas_call(
            functools.partial(kernel, (SP, TP)),
            out_shape=jax.ShapeDtypeStruct((count, width), BF16),
            in_specs=[vmem] * 10 + [hbm] + [vmem] * 5 + [hbm] * 3,
            out_specs=vmem,
            scratch_shapes=[
                pltpu.VMEM((2, n + 16, n), BF16),
                pltpu.VMEM((n + 16, n), BF16),
                pltpu.VMEM((4, n + 16, n), BF16),
                pltpu.VMEM((3, n + 16, n), BF16),
                pltpu.VMEM((2, n // 2 + 16, n), BF16),
                pltpu.VMEM((2, n // 2, n), BF16),
                pltpu.VMEM((TP, count, channels), BF16),
                pltpu.VMEM((TP, count, channels), BF16),
                pltpu.VMEM((SP, 1, 128), F32),
                pltpu.VMEM((SP, 1, 128), F32),
                pltpu.VMEM((size, QUARTERS * count), BF16),
                pltpu.VMEM((size, quarter), BF16),
                pltpu.VMEM((size, quarter), BF16),
                pltpu.VMEM((size, channels), BF16),
                pltpu.VMEM((size, channels), BF16),
                pltpu.VMEM((CHUNKS, QUARTERS * TP * taken, chunk), BF16),
                pltpu.VMEM((CHUNKS, chunk, QUARTERS * TP * taken), BF16),
                pltpu.VMEM((CHUNKS, chunk, QUARTERS * TP * taken), BF16),
                pltpu.VMEM((CHUNKS, TP, taken, width), BF16),
                pltpu.VMEM((CHUNKS, TP, taken, width), BF16),
                pltpu.VMEM((CHUNKS, TP, taken, TP * channels), BF16),
                pltpu.VMEM((CHUNKS, TP, taken, TP * channels), BF16),
                pltpu.VMEM((CHUNKS, TP, taken, width), BF16),
                pltpu.VMEM((CHUNKS, TP, taken, width), BF16),
                pltpu.VMEM((size, quarter), BF16),
                pltpu.VMEM((size, quarter), BF16),
                pltpu.VMEM((TP, channels, width), BF16),
                pltpu.VMEM((width, hidden_units), BF16),
                pltpu.VMEM((width, hidden_units), BF16),
                pltpu.VMEM((hidden_units, width), BF16),
                dma((4,)), dma((4,)), dma((4,)), dma((4,)), dma((3,)), dma((3,)),
                dma((TP,)), dma((TP,)), dma((TP,)), dma((TP,)), dma((SP,)), dma((SP,)), dma((SP,)), dma((SP,)),
                dma((SP,)), dma((SP,)), dma((CHUNKS * TP,)), dma((CHUNKS * TP,)), dma((CHUNKS * TP,)),
                dma((CHUNKS * TP,)), dma((CHUNKS * TP,)), dma((CHUNKS * TP,)),
                dma((SP,)), dma((SP,)),
            ],
            compiler_params=pltpu.CompilerParams(
                collective_id=0, has_side_effects=True, vmem_limit_bytes=56 * 1024 * 1024
            ),
        )(
            receptance, key_matrix, value_matrix, output_gate_logits, onward_decay_logits, reverse_decay_logits,
            correction_rate_logits, extra_log_decay.T, documents.reshape(1, n), head_norm_scale.reshape(1, channels),
            mixer_output_weight, residual, expert_norm_scale.reshape(1, width), expert_choice_index.T,
            group_route_weight.reshape(1, count), expert_route_weight.T,
            expert_gate_matrix[0], expert_up_matrix[0], expert_down_matrix[0],
        )

    in_specs = (
        (P(GRP_SP, "tp"),) * 8
        + (P(GRP_SP), P("tp"), P("tp", None), P(GRP_SP_TP, None), P(), P(GRP_SP_TP, None))
        + (P(GRP_SP_TP), P(GRP_SP_TP, None))
        + (P(SP_TP, None, None),) * 3
    )
    return jax.shard_map(
        body, mesh=mesh, in_specs=in_specs, out_specs=P(GRP_SP_TP, None), check_vma=False
    )
```

```python
import functools

import jax
import jax.numpy as jnp
from jax import lax
from jax.experimental import pallas as pl
from jax.experimental.pallas import tpu as pltpu
from jax.sharding import PartitionSpec as P

HEAD_DIM = 64
GRP_SP = ("grp", "sp")
GRP_SP_TP = ("grp", "sp", "tp")
SP_TP = ("sp", "tp")
MESH = pl.DeviceIdType.MESH
HIGHEST = lax.Precision.HIGHEST
F32 = jnp.float32
BF16 = jnp.bfloat16
QUARTERS = 4
SLOTS = 4
GROUP = 4
CAP = 2
CHUNKS = 4
REACH = 4


def dot(a, b, dims=((1,), (0,)), precision=None):
    return lax.dot_general(a, b, (dims, ((), ())), preferred_element_type=F32, precision=precision)


def low(a, b, dims=((1,), (0,))):
    return dot(a.astype(BF16), b.astype(BF16), dims)


ROWS = ((0,), (0,))
LANES = ((1,), (1,))


def iota(shape, dim):
    return lax.broadcasted_iota(jnp.int32, shape, dim)


def sigmoid(x):
    return 1.0 / (1.0 + jnp.exp(-x))


def inverse(lower, row, col):
    eye = (row == col).astype(F32)
    near = jnp.where((row >> 3) == (col >> 3), lower, 0.0)
    second = dot(near, near, precision=HIGHEST)
    fourth = dot(second, second, precision=HIGHEST)
    found = dot(eye - near, eye + second, precision=HIGHEST)
    found = dot(found, eye + fourth, precision=HIGHEST)
    bit = 3
    while (1 << bit) < lower.shape[0]:
        across = ((row >> (bit + 1)) == (col >> (bit + 1))) & ((row >> bit) != (col >> bit))
        found = found - low(low(found, jnp.where(across, lower, 0.0)), found)
        bit += 1
    return found


def column_of(line, eye):
    return jnp.sum(jnp.where(eye, line, jnp.zeros_like(line)), axis=1, keepdims=True)


def line_of(column, eye):
    return jnp.sum(jnp.where(eye, column, jnp.zeros_like(column)), axis=0, keepdims=True)


def direction(reader, keys, values, unit, rates, log_decay, doc_col, doc_row, back):
    n = reader.shape[0]
    row, col = iota((n, n), 0), iota((n, n), 1)
    lane = iota((1, n), 1)
    first_head = lane < HEAD_DIM
    same_head = (row < HEAD_DIM) == (col < HEAD_DIM)
    upto = (col >= row) if back else (col <= row)
    match = doc_col == doc_row
    inclusive = upto & match
    strict = inclusive & (row != col)
    running = dot(upto.astype(F32), log_decay, precision=HIGHEST)
    total = running[:1] if back else running[n - 1 :]
    middle = 0.5 * total
    before = running - log_decay
    head_doc = doc_row[:, n - 1 :] if back else doc_row[:, :1]
    tail_doc = doc_row[:, :1] if back else doc_row[:, n - 1 :]
    opened = (doc_col == head_doc).astype(F32)
    closing = (doc_col == tail_doc).astype(F32)
    probe = unit * jnp.exp(before - middle)
    lifted = reader * jnp.exp(running - middle)
    undo = jnp.exp(middle - running)
    fix_keys = rates * unit * undo
    add_keys = keys * undo
    rest = jnp.exp(total - running)
    fix_last = rates * unit * rest
    add_last = keys * rest
    probe_open = opened * unit * jnp.exp(before)
    lifted_open = opened * reader * jnp.exp(running)
    left = jnp.concatenate([probe, lifted], axis=0)
    right = jnp.concatenate([fix_keys, add_keys], axis=0).astype(BF16)
    values_low = values.astype(BF16)
    removed, added, reads = [], [], []
    for head in range(2):
        mine = first_head if head == 0 else jnp.logical_not(first_head)
        grams = low(jnp.where(mine, left, 0.0), right, LANES)
        system = jnp.where(strict, grams[:n, :n], 0.0)
        add_mix = jnp.where(strict, grams[:n, n:], 0.0)
        reads.append(jnp.where(inclusive, grams[n:, :n], 0.0))
        read_add = jnp.where(inclusive, grams[n:, n:], 0.0)
        mixed = low(jnp.concatenate([add_mix, read_add], axis=0), values_low)
        added.append(mixed[n:])
        source = -jnp.concatenate([mixed[:n], probe_open], axis=1)
        removed.append(low(inverse(system, row, col), source))
    both = jnp.concatenate([first_head, first_head], axis=1)
    took = jnp.where(both, removed[0], removed[1])
    heads = [low(reads[head], took) for head in range(2)]
    through = jnp.where(both, heads[0], heads[1])
    outputs = through[:, :n] + jnp.where(first_head, added[0], added[1])
    response = through[:, n:] + lifted_open
    ends = low(took * closing, fix_last, ROWS)
    add = ends[:n] + low(values * closing, add_last, ROWS)
    whole = (head_doc == tail_doc).astype(F32)
    keep = ends[n:] + jnp.where(row == col, whole * jnp.exp(total), 0.0)
    add = jnp.where(same_head, add, 0.0)
    keep = jnp.where(same_head, keep, 0.0)
    half = n // 2
    element = jnp.concatenate(
        [
            keep[:half] + keep[half:],
            add[:half] + add[half:],
            jnp.broadcast_to(head_doc, (8, n)),
            jnp.broadcast_to(tail_doc, (8, n)),
        ],
        axis=0,
    ).astype(BF16)
    return outputs, response, element


def spread(block, same_head):
    return jnp.where(same_head, jnp.concatenate([block, block], axis=0), jnp.zeros_like(same_head, block.dtype))


def link(tail, head):
    return (tail == head).astype(F32)


def kernel(sizes, *refs):
    (
        receptance_ref, key_ref, value_ref, out_gate_ref, onward_ref, reverse_ref, rate_ref, extra_ref,
        docs_ref, head_scale_ref, mixer_hbm, residual_ref, expert_scale_ref, choice_ref, group_weight_ref,
        route_ref, gate_hbm, up_hbm, down_hbm,
        updated_ref,
        element, partner, chip, came, far, entering,
        mix_out, mixes, meta_out, meta_in, place, packed, arrived, pick, weigh_hi, weigh_lo,
        outward, inbound, answers, answered, combined, returned,
        mixer_w, gate_w, up_w, down_w,
        w_sem, pair_sem, scan_send, scan_recv, mixer_send, mixer_recv, share_send, share_recv,
        mix_send, mix_recv, meta_send, meta_recv, out_send, out_recv, x_send, x_recv, y_send, y_recv,
        back_send, back_recv,
    ) = refs
    SP, TP = sizes
    chips = SP // 2
    sp, tp = lax.axis_index("sp"), lax.axis_index("tp")
    z, core = lax.div(sp, 2), lax.rem(sp, 2)
    n = receptance_ref.shape[0]
    count, width = residual_ref.shape
    quarter = width // QUARTERS
    piece = QUARTERS * SLOTS
    size = SP * piece
    group_slots = SP // CHUNKS
    chunk = group_slots * piece
    taken = group_slots * CAP

    barrier = pltpu.get_barrier_semaphore()

    def greet_sp(o, carry):
        pl.semaphore_signal(barrier, inc=1, device_id={"sp": lax.rem(sp + o, SP)}, device_id_type=MESH)
        return carry

    lax.fori_loop(1, SP, greet_sp, 0)
    for o in range(1, TP):
        pl.semaphore_signal(barrier, inc=1, device_id={"tp": lax.rem(tp + o, TP)}, device_id_type=MESH)

    loads = [
        pltpu.make_async_copy(src, dst, w_sem.at[k])
        for k, (src, dst) in enumerate(
            ((mixer_hbm, mixer_w.at[tp]), (gate_hbm, gate_w), (up_hbm, up_w), (down_hbm, down_w))
        )
    ]
    for load in loads:
        load.start()

    def turn(k):
        half = (k + 1) >> 1
        if isinstance(k, int):
            return SP // 2 + (-half if k & 1 else half)
        return SP // 2 + jnp.where((k & 1) == 1, -half, half)

    def ahead(k):
        peer = sp + turn(k)
        return jnp.where(peer >= SP, peer - SP, peer)

    def behind(k):
        peer = sp - turn(k)
        return jnp.where(peer < 0, peer + SP, peer)

    def sp_copy(src, dst, send, recv, k, back=False):
        return pltpu.make_async_remote_copy(
            src_ref=src, dst_ref=dst, send_sem=send.at[k], recv_sem=recv.at[k],
            device_id={"sp": behind(k) if back else ahead(k)}, device_id_type=MESH,
        )

    def rows_at(ref, k):
        return ref.at[pl.ds(pl.multiple_of(k * piece, piece), piece)]

    def meta_copy(k):
        return sp_copy(meta_out.at[k], meta_in.at[k], meta_send, meta_recv, k)

    def out_copy(k):
        return sp_copy(rows_at(packed, k), rows_at(arrived, k), out_send, out_recv, k)

    def home_copy(k):
        return sp_copy(rows_at(combined, k), rows_at(returned, k), back_send, back_recv, k, True)

    def begin(copy):
        copy.start()

    def each(make, act, first=0, last=SP - 1):
        if act is begin:
            for k in range(first, last):
                act(make(k))
            return

        def one(k, carry):
            act(make(k))
            return carry

        lax.fori_loop(first, last, one, 0)

    def leave(copy):
        copy.wait_send()

    def arrive(copy):
        copy.wait_recv()

    def bounds(c):
        return c * group_slots, min((c + 1) * group_slots, SP - 1)

    def tp_copy(src, dst, send, recv, k, o):
        return pltpu.make_async_remote_copy(
            src_ref=src, dst_ref=dst, send_sem=send.at[k], recv_sem=recv.at[k],
            device_id={"tp": lax.rem(tp + o, TP)}, device_id_type=MESH,
        )

    row, col = iota((n, n), 0), iota((n, n), 1)
    eye = row == col
    same_head = (row < HEAD_DIM) == (col < HEAD_DIM)
    first_head = iota((1, n), 1) < HEAD_DIM
    doc_row = docs_ref[...].astype(F32)
    doc_col = column_of(doc_row, eye)
    reader = receptance_ref[...].astype(F32)
    keys = key_ref[...].astype(F32)
    values = value_ref[...].astype(F32)

    def by_head(x):
        one = jnp.sum(jnp.where(first_head, x, 0.0), axis=1, keepdims=True)
        two = jnp.sum(jnp.where(first_head, 0.0, x), axis=1, keepdims=True)
        return jnp.where(first_head, one, two)

    unit = keys * lax.rsqrt(by_head(keys * keys) + 1e-06)
    rates = sigmoid(rate_ref[...].astype(F32))
    extra = jnp.where(first_head, column_of(extra_ref[:1], eye), column_of(extra_ref[1:2], eye))
    level = 0.6065306597126334
    onward = -level * sigmoid(onward_ref[...].astype(F32)) + extra
    reverse = -level * sigmoid(reverse_ref[...].astype(F32)) + extra
    out_f, resp_f, element_f = direction(reader, keys, values, unit, rates, onward, doc_col, doc_row, False)
    out_b, resp_b, element_b = direction(reader, keys, values, unit, rates, reverse, doc_col, doc_row, True)
    element[0] = element_f
    element[1] = element_b

    sign = 1 - 2 * core

    def pair_copy(src, dst, k):
        return pltpu.make_async_remote_copy(
            src_ref=src, dst_ref=dst, send_sem=pair_sem.at[2 * k], recv_sem=pair_sem.at[2 * k + 1],
            device_id={"sp": sp + sign}, device_id_type=MESH,
        )

    def chip_peer(distance):
        return lax.rem(z + sign * distance + chips, chips) * 2 + core

    def exists(distance):
        origin = z - sign * distance
        return (origin >= 0) & (origin < chips)

    half = n // 2

    def parts(ref_value):
        value = ref_value.astype(F32)
        return value[:half], value[half : 2 * half], value[n : n + 1], value[n + 8 : n + 9]

    pl.semaphore_wait(barrier, SP - 1 + TP - 1)
    first_copy = pair_copy(element.at[1 - core], partner, 0)
    first_copy.start()

    half_rows = n // 2
    own_rows = pl.ds(pl.multiple_of(core * half_rows, half_rows), half_rows)

    def block(o):
        return mixer_w.at[lax.rem(tp + o + TP, TP), own_rows]

    def round_copy(k):
        o, src = ((1, block(0)), (TP - 1, block(0)), (jnp.where(core == 0, 1, TP - 1), block(jnp.where(core == 0, -1, 1))))[k]
        return tp_copy(src, src, mixer_send, mixer_recv, k, o)

    def give_copy(o):
        src = block(o)
        return pltpu.make_async_remote_copy(
            src_ref=src, dst_ref=src, send_sem=share_send.at[o], recv_sem=share_recv.at[o],
            device_id={"sp": sp + sign}, device_id_type=MESH,
        )

    loads[0].wait()
    round_copy(0).start()
    round_copy(1).start()
    first_copy.wait()
    own = element[core].astype(F32)
    own_keep, own_add, own_head, own_tail = own[:half], own[half:n], own[n : n + 1], own[n + 8 : n + 9]
    par_keep, par_add, par_head, par_tail = parts(partner[...])
    joined = link(own_tail, par_head)
    both = joined * low(own[:n], spread(par_keep, same_head))
    def keep_element(at, both, head, tail):
        chip[at] = jnp.concatenate(
            [both, jnp.broadcast_to(head, (8, n)), jnp.broadcast_to(tail, (8, n))], axis=0
        ).astype(BF16)

    zeros = jnp.zeros((half, n), F32)
    window = both + jnp.concatenate([zeros, par_add], axis=0)
    head, tail = own_head, par_tail

    def scan_copy(k):
        src, dst, distance = (
            (chip.at[0], came.at[0], 1),
            (chip.at[1], came.at[1], 2),
            (chip.at[2], came.at[2], 1),
            (far.at[0], far.at[1], REACH + 1),
        )[k]
        return pltpu.make_async_remote_copy(
            src_ref=src, dst_ref=dst, send_sem=scan_send.at[k], recv_sem=scan_recv.at[k],
            device_id={"sp": chip_peer(distance)}, device_id_type=MESH,
        )

    def doubled(k, distance, window, head):
        past_keep, past_add, past_head, past_tail = parts(came[k])
        past_tail = jnp.where(exists(distance), past_tail, -1.0)
        joined = link(past_tail, head) * low(
            jnp.concatenate([past_keep, past_add], axis=0), spread(window[:half], same_head)
        )
        return joined + jnp.concatenate([zeros, window[half:]], axis=0), past_head

    keep_element(0, window, head, tail)
    scan_copy(0).start()

    lane32, row32 = iota((count, count), 1), iota((count, count), 0)
    eye32 = lane32 == row32
    choice = choice_ref[...].astype(F32)
    lead_line, trail_line = choice[:1], choice[1:2]
    lead, trail = column_of(lead_line, eye32), column_of(trail_line, eye32)
    lead_group = jnp.floor(lead * (1.0 / GROUP))
    group_line = line_of(lead_group, eye32)
    earlier = lane32 < row32

    def rank(mask):
        return jnp.sum(jnp.where(earlier & mask, 1.0, 0.0), axis=1, keepdims=True)

    slot = rank(lead_group == group_line)
    lead_rank = rank((lead == lead_line) | (lead == trail_line))
    trail_rank = rank((trail == lead_line) | (trail == trail_line))
    first_weight, second_weight = column_of(route_ref[:1], eye32), column_of(route_ref[1:2], eye32)
    scale = column_of(group_weight_ref[...], eye32) / (first_weight + second_weight)
    lane = iota((count, 128), 1).astype(F32)
    lead_own = lead - GROUP * lead_group + 2 * GROUP * slot
    trail_own = trail - GROUP * lead_group + 2 * GROUP * slot
    info = (
        jnp.where(lane == lead_own, lead_rank + 1.0, 0.0)
        + jnp.where(lane == trail_own, trail_rank + 1.0, 0.0)
        + jnp.where(lane == lead_own + GROUP, scale * first_weight, 0.0)
        + jnp.where(lane == trail_own + GROUP, scale * second_weight, 0.0)
    )
    goes = (ahead(iota((SP, count), 0)).astype(F32) == group_line).astype(F32)
    meta_out[...] = dot(goes, info, precision=HIGHEST).reshape(SP, 1, 128)
    each(meta_copy, begin)
    meta_in[SP - 1] = meta_out[SP - 1]
    stacked = QUARTERS * count
    group4, slot4 = jnp.concatenate([lead_group] * QUARTERS, 0), jnp.concatenate([slot] * QUARTERS, 0)
    at, at_row = iota((stacked, size), 1), iota((stacked, size), 0)
    table = (
        (group4 == ahead(at >> 4).astype(F32))
        & (slot4 == (at & 3).astype(F32))
        & (lax.div(at_row, count) == ((at >> 2) & 3))
    ).astype(F32)
    place[...] = table.T.astype(BF16)
    table = table.astype(BF16)
    scan_copy(0).wait_recv()
    window, head = doubled(0, 1, window, head)
    keep_element(1, window, head, tail)
    scan_copy(1).start()
    round_copy(0).wait_recv()
    round_copy(1).wait_recv()
    round_copy(2).start()
    scan_copy(1).wait_recv()
    window, head = doubled(1, 2, window, head)
    far[0] = jnp.concatenate([window[half:], jnp.broadcast_to(tail, (16, n))], axis=0).astype(BF16)
    scan_copy(3).start()
    keep_element(2, window, head, tail)
    scan_copy(2).start()
    round_copy(2).wait_recv()
    for o in range(1, TP):
        give_copy(o).start()
    scan_copy(2).wait_recv()
    keep, add, past_head, past_tail = parts(came[2])
    keep = spread(keep, same_head)
    scan_copy(3).wait_recv()
    far_value = far[1].astype(F32)
    far_tail = jnp.where(exists(REACH + 1), far_value[half : half + 1], -1.0)
    add = add + link(far_tail, past_head) * low(far_value[:half], keep)
    tail = jnp.where(exists(1), past_tail, -1.0)
    state = link(tail, own_head) * add
    passed = (low(state, spread(own_keep, same_head)) + own_add) * joined
    entering[0] = passed.astype(BF16)
    last_copy = pair_copy(entering.at[0], entering.at[1], 1)
    last_copy.start()
    last_copy.wait()
    other = entering[1].astype(F32)
    state_f = jnp.where(core == 0, state, other)
    state_b = jnp.where(core == 0, other, state)
    entry = jnp.concatenate([spread(state_f, same_head), spread(state_b, same_head)], axis=1)
    mixed = out_f + out_b + low(jnp.concatenate([resp_f, resp_b], axis=1), entry, LANES)

    centred = mixed - by_head(mixed) * (1.0 / HEAD_DIM)
    scaled = centred * lax.rsqrt(by_head(centred * centred) * (1.0 / HEAD_DIM) + 0.00064)
    mix = (scaled * head_scale_ref[...] * sigmoid(out_gate_ref[...].astype(F32))).astype(BF16)
    for o in range(TP):
        mix_out[o] = mix[o * count : (o + 1) * count]

    def mix_copy(o):
        return tp_copy(mix_out.at[lax.rem(tp + o, TP)], mixes.at[tp], mix_send, mix_recv, o, o)

    for o in (2, 1, 3):
        mix_copy(o).start()
    mixes[tp] = mix_out[tp]
    for o in range(1, TP):
        give_copy(o).wait_recv()
    residual = residual_ref[...].astype(F32)
    for o in (1, 3, 2):
        mix_copy(o).wait_recv()
    wide = jnp.concatenate([mixes[o] for o in range(TP)], axis=1)
    hidden = residual + dot(wide, mixer_w[...].reshape(TP * n, width))
    hidden = hidden.astype(BF16).astype(F32)
    normed = (
        hidden * lax.rsqrt(jnp.mean(hidden * hidden, axis=1, keepdims=True) + 1e-06) * expert_scale_ref[...]
    ).astype(BF16)

    quarters = jnp.concatenate([normed[:, q * quarter : (q + 1) * quarter] for q in range(QUARTERS)], axis=0)
    packed[...] = dot(place[...], quarters).astype(BF16)
    each(out_copy, begin)
    arrived[size - piece :] = packed[size - piece :]

    each(meta_copy, arrive)
    told = meta_in[...].reshape(SP, 128)
    lane = iota((chunk, 128), 1)
    slot_lane = (iota((chunk, 128), 0) & 3) * (2 * GROUP)
    cols = QUARTERS * TP * taken
    row, col = iota((chunk, cols), 0), iota((chunk, cols), 1)
    col_q, col_o = lax.div(col, TP * taken), lax.rem(lax.div(col, taken), TP)
    col_k, col_e = lax.rem(lax.div(col, CAP), group_slots), (col & 1) + 1
    same_place = ((row >> 4) == col_k) & (((row >> 2) & 3) == col_q)
    source_row, source_col = iota((chunk, SP), 0), iota((chunk, SP), 1)
    for c in range(CHUNKS):
        widen = ((source_row >> 4) + c * group_slots == source_col).astype(F32)
        meta = dot(widen, told, precision=HIGHEST)
        codes, weights = jnp.zeros((chunk, cols), F32), jnp.zeros((chunk, cols), F32)
        for o in range(TP):
            at_code = slot_lane + lax.rem(tp + o, TP)
            code = jnp.sum(jnp.where(lane == at_code, meta, 0.0), axis=1, keepdims=True)
            weight = jnp.sum(jnp.where(lane == at_code + GROUP, meta, 0.0), axis=1, keepdims=True)
            codes, weights = jnp.where(col_o == o, code, codes), jnp.where(col_o == o, weight, weights)
        hit = same_place & (codes == col_e.astype(F32))
        pick[c] = jnp.where(hit, 1.0, 0.0).T.astype(BF16)
        weights = jnp.where(hit, weights, 0.0)
        high = weights.astype(BF16)
        weigh_hi[c] = high
        weigh_lo[c] = (weights - high.astype(F32)).astype(BF16)

    def to_expert(c, o):
        return tp_copy(outward.at[c, o], inbound.at[c, o], x_send, x_recv, c * TP + o, o)

    def from_expert(c, o):
        return tp_copy(answers.at[c, o], answered.at[c, o], y_send, y_recv, c * TP + o, TP - o)

    def take(c):
        each(out_copy, arrive, *bounds(c))
        rows = dot(pick[c], arrived[c * chunk : (c + 1) * chunk]).astype(BF16)
        for o in (2, 1, 3, 0):
            target = outward if o else inbound
            for q in range(QUARTERS):
                first = (q * TP + o) * taken
                target[c, o, :, q * quarter : (q + 1) * quarter] = rows[first : first + taken]
            if o:
                to_expert(c, o).start()

    def work(c):
        for o in (1, 3, 2):
            to_expert(c, o).wait_recv()
        rows = inbound[c].reshape(TP * taken, width)
        gate = dot(rows, gate_w[...])
        up = dot(rows, up_w[...])
        active = (gate * sigmoid(gate) * up).astype(BF16)
        result = dot(active, down_w[...]).astype(BF16)
        for o in (2, 1, 3, 0):
            target = answers if o else answered
            target[c, o] = result[o * taken : (o + 1) * taken]
            if o:
                from_expert(c, o).start()

    def give(c):
        for o in (1, 3, 2):
            from_expert(c, o).wait_recv()
        flat = answered[c].reshape(TP * taken, width)
        flat = jnp.concatenate([flat[:, q * quarter : (q + 1) * quarter] for q in range(QUARTERS)], axis=0)
        at = slice(c * chunk, (c + 1) * chunk)
        combined[at] = (dot(weigh_hi[c], flat) + dot(weigh_lo[c], flat)).astype(BF16)
        each(home_copy, begin, *bounds(c))

    for load in loads[1:]:
        load.wait()
    take(0)
    work(0)
    take(1)
    give(0)
    take(2)
    take(3)
    work(1)
    work(2)
    work(3)
    give(1)
    give(2)
    give(3)
    returned[size - piece :] = combined[size - piece :]

    for k in range(3):
        round_copy(k).wait_send()
    for k in range(4):
        scan_copy(k).wait_send()
    for o in range(1, TP):
        give_copy(o).wait_send()
        mix_copy(o).wait_send()
        for c in range(CHUNKS):
            to_expert(c, o).wait_send()
            from_expert(c, o).wait_send()
    each(meta_copy, leave)
    each(out_copy, leave)
    final = jnp.zeros((stacked, quarter), F32)
    for c in range(CHUNKS):
        each(home_copy, arrive, *bounds(c))
        at = slice(c * chunk, (c + 1) * chunk)
        final += dot(table[:, at], returned[at])
    for q in range(QUARTERS):
        at = slice(q * quarter, (q + 1) * quarter)
        updated_ref[:, at] = (hidden[:, at] + final[q * count : (q + 1) * count]).astype(BF16)

    each(home_copy, leave)


def solution(mesh):
    SP, TP = mesh.shape["sp"], mesh.shape["tp"]

    def body(
        receptance, key_matrix, value_matrix, output_gate_logits, onward_decay_logits, reverse_decay_logits,
        correction_rate_logits, extra_log_decay, documents, head_norm_scale, mixer_output_weight, residual,
        expert_norm_scale, expert_choice_index, group_route_weight, expert_route_weight,
        expert_gate_matrix, expert_up_matrix, expert_down_matrix,
    ):
        n, channels = receptance.shape
        count, width = residual.shape
        hidden_units = expert_gate_matrix.shape[2]
        piece = QUARTERS * SLOTS
        size, quarter = SP * piece, width // QUARTERS
        chunk, taken = size // CHUNKS, SP // CHUNKS * CAP
        vmem, hbm = pl.BlockSpec(memory_space=pltpu.VMEM), pl.BlockSpec(memory_space=pl.ANY)
        dma = pltpu.SemaphoreType.DMA
        return pl.pallas_call(
            functools.partial(kernel, (SP, TP)),
            out_shape=jax.ShapeDtypeStruct((count, width), BF16),
            in_specs=[vmem] * 10 + [hbm] + [vmem] * 5 + [hbm] * 3,
            out_specs=vmem,
            scratch_shapes=[
                pltpu.VMEM((2, n + 16, n), BF16),
                pltpu.VMEM((n + 16, n), BF16),
                pltpu.VMEM((4, n + 16, n), BF16),
                pltpu.VMEM((3, n + 16, n), BF16),
                pltpu.VMEM((2, n // 2 + 16, n), BF16),
                pltpu.VMEM((2, n // 2, n), BF16),
                pltpu.VMEM((TP, count, channels), BF16),
                pltpu.VMEM((TP, count, channels), BF16),
                pltpu.VMEM((SP, 1, 128), F32),
                pltpu.VMEM((SP, 1, 128), F32),
                pltpu.VMEM((size, QUARTERS * count), BF16),
                pltpu.VMEM((size, quarter), BF16),
                pltpu.VMEM((size, quarter), BF16),
                pltpu.VMEM((CHUNKS, QUARTERS * TP * taken, chunk), BF16),
                pltpu.VMEM((CHUNKS, chunk, QUARTERS * TP * taken), BF16),
                pltpu.VMEM((CHUNKS, chunk, QUARTERS * TP * taken), BF16),
                pltpu.VMEM((CHUNKS, TP, taken, width), BF16),
                pltpu.VMEM((CHUNKS, TP, taken, width), BF16),
                pltpu.VMEM((CHUNKS, TP, taken, width), BF16),
                pltpu.VMEM((CHUNKS, TP, taken, width), BF16),
                pltpu.VMEM((size, quarter), BF16),
                pltpu.VMEM((size, quarter), BF16),
                pltpu.VMEM((TP, channels, width), BF16),
                pltpu.VMEM((width, hidden_units), BF16),
                pltpu.VMEM((width, hidden_units), BF16),
                pltpu.VMEM((hidden_units, width), BF16),
                dma((4,)), dma((4,)), dma((4,)), dma((4,)), dma((3,)), dma((3,)),
                dma((TP,)), dma((TP,)), dma((TP,)), dma((TP,)), dma((SP,)), dma((SP,)), dma((SP,)), dma((SP,)),
                dma((CHUNKS * TP,)), dma((CHUNKS * TP,)), dma((CHUNKS * TP,)), dma((CHUNKS * TP,)),
                dma((SP,)), dma((SP,)),
            ],
            compiler_params=pltpu.CompilerParams(
                collective_id=0, has_side_effects=True, vmem_limit_bytes=56 * 1024 * 1024
            ),
        )(
            receptance, key_matrix, value_matrix, output_gate_logits, onward_decay_logits, reverse_decay_logits,
            correction_rate_logits, extra_log_decay.T, documents.reshape(1, n), head_norm_scale.reshape(1, channels),
            mixer_output_weight, residual, expert_norm_scale.reshape(1, width), expert_choice_index.T,
            group_route_weight.reshape(1, count), expert_route_weight.T,
            expert_gate_matrix[0], expert_up_matrix[0], expert_down_matrix[0],
        )

    in_specs = (
        (P(GRP_SP, "tp"),) * 8
        + (P(GRP_SP), P("tp"), P("tp", None), P(GRP_SP_TP, None), P(), P(GRP_SP_TP, None))
        + (P(GRP_SP_TP), P(GRP_SP_TP, None))
        + (P(SP_TP, None, None),) * 3
    )
    return jax.shard_map(
        body, mesh=mesh, in_specs=in_specs, out_specs=P(GRP_SP_TP, None), check_vma=False
    )
```

```python
import functools

import jax
import jax.numpy as jnp
from jax import lax
from jax.experimental import pallas as pl
from jax.experimental.pallas import tpu as pltpu
from jax.sharding import PartitionSpec as P

HEAD_DIM = 64
GRP_SP = ("grp", "sp")
GRP_SP_TP = ("grp", "sp", "tp")
SP_TP = ("sp", "tp")
MESH = pl.DeviceIdType.MESH
HIGHEST = lax.Precision.HIGHEST
F32 = jnp.float32
BF16 = jnp.bfloat16
QUARTERS = 4
SLOTS = 4
GROUP = 4
CAP = 2
CHUNKS = 8
REACH = 4


def dot(a, b, dims=((1,), (0,)), precision=None):
    return lax.dot_general(a, b, (dims, ((), ())), preferred_element_type=F32, precision=precision)


def low(a, b, dims=((1,), (0,))):
    return dot(a.astype(BF16), b.astype(BF16), dims)


ROWS = ((0,), (0,))
LANES = ((1,), (1,))


def iota(shape, dim):
    return lax.broadcasted_iota(jnp.int32, shape, dim)


def sigmoid(x):
    return 1.0 / (1.0 + jnp.exp(-x))


def inverse(lower, row, col):
    eye = (row == col).astype(F32)
    near = jnp.where((row >> 3) == (col >> 3), lower, 0.0)
    second = dot(near, near, precision=HIGHEST)
    fourth = dot(second, second, precision=HIGHEST)
    found = dot(eye - near, eye + second, precision=HIGHEST)
    found = dot(found, eye + fourth, precision=HIGHEST)
    bit = 3
    while (1 << bit) < lower.shape[0]:
        across = ((row >> (bit + 1)) == (col >> (bit + 1))) & ((row >> bit) != (col >> bit))
        found = found - low(low(found, jnp.where(across, lower, 0.0)), found)
        bit += 1
    return found


def column_of(line, eye):
    return jnp.sum(jnp.where(eye, line, jnp.zeros_like(line)), axis=1, keepdims=True)


def line_of(column, eye):
    return jnp.sum(jnp.where(eye, column, jnp.zeros_like(column)), axis=0, keepdims=True)


def direction(reader, keys, values, unit, rates, log_decay, doc_col, doc_row, back):
    n = reader.shape[0]
    row, col = iota((n, n), 0), iota((n, n), 1)
    lane = iota((1, n), 1)
    first_head = lane < HEAD_DIM
    same_head = (row < HEAD_DIM) == (col < HEAD_DIM)
    upto = (col >= row) if back else (col <= row)
    match = doc_col == doc_row
    inclusive = upto & match
    strict = inclusive & (row != col)
    running = dot(upto.astype(F32), log_decay, precision=HIGHEST)
    total = running[:1] if back else running[n - 1 :]
    middle = 0.5 * total
    before = running - log_decay
    head_doc = doc_row[:, n - 1 :] if back else doc_row[:, :1]
    tail_doc = doc_row[:, :1] if back else doc_row[:, n - 1 :]
    opened = (doc_col == head_doc).astype(F32)
    closing = (doc_col == tail_doc).astype(F32)
    probe = unit * jnp.exp(before - middle)
    lifted = reader * jnp.exp(running - middle)
    undo = jnp.exp(middle - running)
    fix_keys = rates * unit * undo
    add_keys = keys * undo
    rest = jnp.exp(total - running)
    fix_last = rates * unit * rest
    add_last = keys * rest
    probe_open = opened * unit * jnp.exp(before)
    lifted_open = opened * reader * jnp.exp(running)
    left = jnp.concatenate([probe, lifted], axis=0)
    right = jnp.concatenate([fix_keys, add_keys], axis=0).astype(BF16)
    values_low = values.astype(BF16)
    removed, added, reads = [], [], []
    for head in range(2):
        mine = first_head if head == 0 else jnp.logical_not(first_head)
        grams = low(jnp.where(mine, left, 0.0), right, LANES)
        system = jnp.where(strict, grams[:n, :n], 0.0)
        add_mix = jnp.where(strict, grams[:n, n:], 0.0)
        reads.append(jnp.where(inclusive, grams[n:, :n], 0.0))
        read_add = jnp.where(inclusive, grams[n:, n:], 0.0)
        mixed = low(jnp.concatenate([add_mix, read_add], axis=0), values_low)
        added.append(mixed[n:])
        source = -jnp.concatenate([mixed[:n], probe_open], axis=1)
        removed.append(low(inverse(system, row, col), source))
    both = jnp.concatenate([first_head, first_head], axis=1)
    took = jnp.where(both, removed[0], removed[1])
    heads = [low(reads[head], took) for head in range(2)]
    through = jnp.where(both, heads[0], heads[1])
    outputs = through[:, :n] + jnp.where(first_head, added[0], added[1])
    response = through[:, n:] + lifted_open
    ends = low(took * closing, fix_last, ROWS)
    add = ends[:n] + low(values * closing, add_last, ROWS)
    whole = (head_doc == tail_doc).astype(F32)
    keep = ends[n:] + jnp.where(row == col, whole * jnp.exp(total), 0.0)
    add = jnp.where(same_head, add, 0.0)
    keep = jnp.where(same_head, keep, 0.0)
    half = n // 2
    element = jnp.concatenate(
        [
            keep[:half] + keep[half:],
            add[:half] + add[half:],
            jnp.broadcast_to(head_doc, (8, n)),
            jnp.broadcast_to(tail_doc, (8, n)),
        ],
        axis=0,
    ).astype(BF16)
    return outputs, response, element


def spread(block, same_head):
    return jnp.where(same_head, jnp.concatenate([block, block], axis=0), jnp.zeros_like(same_head, block.dtype))


def link(tail, head):
    return (tail == head).astype(F32)


def kernel(sizes, *refs):
    (
        receptance_ref, key_ref, value_ref, out_gate_ref, onward_ref, reverse_ref, rate_ref, extra_ref,
        docs_ref, head_scale_ref, mixer_hbm, residual_ref, expert_scale_ref, choice_ref, group_weight_ref,
        route_ref, gate_hbm, up_hbm, down_hbm,
        updated_ref,
        element, partner, chip, came, far, entering,
        mix_out, mixes, meta_out, meta_in, place, packed, arrived, pick, weigh_hi, weigh_lo,
        outward, inbound, answers, answered, combined, returned,
        mixer_w, gate_w, up_w, down_w,
        w_sem, pair_sem, scan_send, scan_recv, mixer_send, mixer_recv, share_send, share_recv,
        mix_send, mix_recv, meta_send, meta_recv, out_send, out_recv, x_send, x_recv, y_send, y_recv,
        back_send, back_recv,
    ) = refs
    SP, TP = sizes
    chips = SP // 2
    sp, tp = lax.axis_index("sp"), lax.axis_index("tp")
    z, core = lax.div(sp, 2), lax.rem(sp, 2)
    n = receptance_ref.shape[0]
    count, width = residual_ref.shape
    quarter = width // QUARTERS
    piece = QUARTERS * SLOTS
    size = SP * piece
    group_slots = SP // CHUNKS
    chunk = group_slots * piece
    taken = group_slots * CAP

    barrier = pltpu.get_barrier_semaphore()

    def greet_sp(o, carry):
        pl.semaphore_signal(barrier, inc=1, device_id={"sp": lax.rem(sp + o, SP)}, device_id_type=MESH)
        return carry

    lax.fori_loop(1, SP, greet_sp, 0)
    for o in range(1, TP):
        pl.semaphore_signal(barrier, inc=1, device_id={"tp": lax.rem(tp + o, TP)}, device_id_type=MESH)

    loads = [
        pltpu.make_async_copy(src, dst, w_sem.at[k])
        for k, (src, dst) in enumerate(
            ((mixer_hbm, mixer_w.at[tp]), (gate_hbm, gate_w), (up_hbm, up_w), (down_hbm, down_w))
        )
    ]
    for load in loads:
        load.start()

    def turn(k):
        half = (k + 1) >> 1
        if isinstance(k, int):
            return SP // 2 + (-half if k & 1 else half)
        return SP // 2 + jnp.where((k & 1) == 1, -half, half)

    def ahead(k):
        peer = sp + turn(k)
        return jnp.where(peer >= SP, peer - SP, peer)

    def behind(k):
        peer = sp - turn(k)
        return jnp.where(peer < 0, peer + SP, peer)

    def sp_copy(src, dst, send, recv, k, back=False):
        return pltpu.make_async_remote_copy(
            src_ref=src, dst_ref=dst, send_sem=send.at[k], recv_sem=recv.at[k],
            device_id={"sp": behind(k) if back else ahead(k)}, device_id_type=MESH,
        )

    def rows_at(ref, k):
        return ref.at[pl.ds(pl.multiple_of(k * piece, piece), piece)]

    def meta_copy(k):
        return sp_copy(meta_out.at[k], meta_in.at[k], meta_send, meta_recv, k)

    def out_copy(k):
        return sp_copy(rows_at(packed, k), rows_at(arrived, k), out_send, out_recv, k)

    def home_copy(k):
        return sp_copy(rows_at(combined, k), rows_at(returned, k), back_send, back_recv, k, True)

    def begin(copy):
        copy.start()

    def each(make, act, first=0, last=SP - 1):
        if act is begin:
            for k in range(first, last):
                act(make(k))
            return

        def one(k, carry):
            act(make(k))
            return carry

        lax.fori_loop(first, last, one, 0)

    def leave(copy):
        copy.wait_send()

    def arrive(copy):
        copy.wait_recv()

    def bounds(c):
        return c * group_slots, min((c + 1) * group_slots, SP - 1)

    def tp_copy(src, dst, send, recv, k, o):
        return pltpu.make_async_remote_copy(
            src_ref=src, dst_ref=dst, send_sem=send.at[k], recv_sem=recv.at[k],
            device_id={"tp": lax.rem(tp + o, TP)}, device_id_type=MESH,
        )

    row, col = iota((n, n), 0), iota((n, n), 1)
    eye = row == col
    same_head = (row < HEAD_DIM) == (col < HEAD_DIM)
    first_head = iota((1, n), 1) < HEAD_DIM
    doc_row = docs_ref[...].astype(F32)
    doc_col = column_of(doc_row, eye)
    reader = receptance_ref[...].astype(F32)
    keys = key_ref[...].astype(F32)
    values = value_ref[...].astype(F32)

    def by_head(x):
        one = jnp.sum(jnp.where(first_head, x, 0.0), axis=1, keepdims=True)
        two = jnp.sum(jnp.where(first_head, 0.0, x), axis=1, keepdims=True)
        return jnp.where(first_head, one, two)

    unit = keys * lax.rsqrt(by_head(keys * keys) + 1e-06)
    rates = sigmoid(rate_ref[...].astype(F32))
    extra = jnp.where(first_head, column_of(extra_ref[:1], eye), column_of(extra_ref[1:2], eye))
    level = 0.6065306597126334
    onward = -level * sigmoid(onward_ref[...].astype(F32)) + extra
    reverse = -level * sigmoid(reverse_ref[...].astype(F32)) + extra
    out_f, resp_f, element_f = direction(reader, keys, values, unit, rates, onward, doc_col, doc_row, False)
    out_b, resp_b, element_b = direction(reader, keys, values, unit, rates, reverse, doc_col, doc_row, True)
    element[0] = element_f
    element[1] = element_b

    sign = 1 - 2 * core

    def pair_copy(src, dst, k):
        return pltpu.make_async_remote_copy(
            src_ref=src, dst_ref=dst, send_sem=pair_sem.at[2 * k], recv_sem=pair_sem.at[2 * k + 1],
            device_id={"sp": sp + sign}, device_id_type=MESH,
        )

    def chip_peer(distance):
        return lax.rem(z + sign * distance + chips, chips) * 2 + core

    def exists(distance):
        origin = z - sign * distance
        return (origin >= 0) & (origin < chips)

    half = n // 2

    def parts(ref_value):
        value = ref_value.astype(F32)
        return value[:half], value[half : 2 * half], value[n : n + 1], value[n + 8 : n + 9]

    pl.semaphore_wait(barrier, SP - 1 + TP - 1)
    first_copy = pair_copy(element.at[1 - core], partner, 0)
    first_copy.start()

    half_rows = n // 2
    own_rows = pl.ds(pl.multiple_of(core * half_rows, half_rows), half_rows)

    def block(o):
        return mixer_w.at[lax.rem(tp + o + TP, TP), own_rows]

    def round_copy(k):
        o, src = ((1, block(0)), (TP - 1, block(0)), (jnp.where(core == 0, 1, TP - 1), block(jnp.where(core == 0, -1, 1))))[k]
        return tp_copy(src, src, mixer_send, mixer_recv, k, o)

    def give_copy(o):
        src = block(o)
        return pltpu.make_async_remote_copy(
            src_ref=src, dst_ref=src, send_sem=share_send.at[o], recv_sem=share_recv.at[o],
            device_id={"sp": sp + sign}, device_id_type=MESH,
        )

    loads[0].wait()
    round_copy(0).start()
    round_copy(1).start()
    first_copy.wait()
    own = element[core].astype(F32)
    own_keep, own_add, own_head, own_tail = own[:half], own[half:n], own[n : n + 1], own[n + 8 : n + 9]
    par_keep, par_add, par_head, par_tail = parts(partner[...])
    joined = link(own_tail, par_head)
    both = joined * low(own[:n], spread(par_keep, same_head))
    def keep_element(at, both, head, tail):
        chip[at] = jnp.concatenate(
            [both, jnp.broadcast_to(head, (8, n)), jnp.broadcast_to(tail, (8, n))], axis=0
        ).astype(BF16)

    zeros = jnp.zeros((half, n), F32)
    window = both + jnp.concatenate([zeros, par_add], axis=0)
    head, tail = own_head, par_tail

    def scan_copy(k):
        src, dst, distance = (
            (chip.at[0], came.at[0], 1),
            (chip.at[1], came.at[1], 2),
            (chip.at[2], came.at[2], 1),
            (far.at[0], far.at[1], REACH + 1),
        )[k]
        return pltpu.make_async_remote_copy(
            src_ref=src, dst_ref=dst, send_sem=scan_send.at[k], recv_sem=scan_recv.at[k],
            device_id={"sp": chip_peer(distance)}, device_id_type=MESH,
        )

    def doubled(k, distance, window, head):
        past_keep, past_add, past_head, past_tail = parts(came[k])
        past_tail = jnp.where(exists(distance), past_tail, -1.0)
        joined = link(past_tail, head) * low(
            jnp.concatenate([past_keep, past_add], axis=0), spread(window[:half], same_head)
        )
        return joined + jnp.concatenate([zeros, window[half:]], axis=0), past_head

    keep_element(0, window, head, tail)
    scan_copy(0).start()

    lane32, row32 = iota((count, count), 1), iota((count, count), 0)
    eye32 = lane32 == row32
    choice = choice_ref[...].astype(F32)
    lead_line, trail_line = choice[:1], choice[1:2]
    lead, trail = column_of(lead_line, eye32), column_of(trail_line, eye32)
    lead_group = jnp.floor(lead * (1.0 / GROUP))
    group_line = line_of(lead_group, eye32)
    earlier = lane32 < row32

    def rank(mask):
        return jnp.sum(jnp.where(earlier & mask, 1.0, 0.0), axis=1, keepdims=True)

    slot = rank(lead_group == group_line)
    lead_rank = rank((lead == lead_line) | (lead == trail_line))
    trail_rank = rank((trail == lead_line) | (trail == trail_line))
    first_weight, second_weight = column_of(route_ref[:1], eye32), column_of(route_ref[1:2], eye32)
    scale = column_of(group_weight_ref[...], eye32) / (first_weight + second_weight)
    lane = iota((count, 128), 1).astype(F32)
    lead_own = lead - GROUP * lead_group + 2 * GROUP * slot
    trail_own = trail - GROUP * lead_group + 2 * GROUP * slot
    info = (
        jnp.where(lane == lead_own, lead_rank + 1.0, 0.0)
        + jnp.where(lane == trail_own, trail_rank + 1.0, 0.0)
        + jnp.where(lane == lead_own + GROUP, scale * first_weight, 0.0)
        + jnp.where(lane == trail_own + GROUP, scale * second_weight, 0.0)
    )
    goes = (ahead(iota((SP, count), 0)).astype(F32) == group_line).astype(F32)
    meta_out[...] = dot(goes, info, precision=HIGHEST).reshape(SP, 1, 128)
    each(meta_copy, begin)
    meta_in[SP - 1] = meta_out[SP - 1]
    stacked = QUARTERS * count
    group4, slot4 = jnp.concatenate([lead_group] * QUARTERS, 0), jnp.concatenate([slot] * QUARTERS, 0)
    at, at_row = iota((stacked, size), 1), iota((stacked, size), 0)
    table = (
        (group4 == ahead(at >> 4).astype(F32))
        & (slot4 == (at & 3).astype(F32))
        & (lax.div(at_row, count) == ((at >> 2) & 3))
    ).astype(F32)
    place[...] = table.T.astype(BF16)
    table = table.astype(BF16)
    scan_copy(0).wait_recv()
    window, head = doubled(0, 1, window, head)
    keep_element(1, window, head, tail)
    scan_copy(1).start()
    round_copy(0).wait_recv()
    round_copy(1).wait_recv()
    round_copy(2).start()
    scan_copy(1).wait_recv()
    window, head = doubled(1, 2, window, head)
    far[0] = jnp.concatenate([window[half:], jnp.broadcast_to(tail, (16, n))], axis=0).astype(BF16)
    scan_copy(3).start()
    keep_element(2, window, head, tail)
    scan_copy(2).start()
    round_copy(2).wait_recv()
    for o in range(1, TP):
        give_copy(o).start()
    scan_copy(2).wait_recv()
    keep, add, past_head, past_tail = parts(came[2])
    keep = spread(keep, same_head)
    scan_copy(3).wait_recv()
    far_value = far[1].astype(F32)
    far_tail = jnp.where(exists(REACH + 1), far_value[half : half + 1], -1.0)
    add = add + link(far_tail, past_head) * low(far_value[:half], keep)
    tail = jnp.where(exists(1), past_tail, -1.0)
    state = link(tail, own_head) * add
    passed = (low(state, spread(own_keep, same_head)) + own_add) * joined
    entering[0] = passed.astype(BF16)
    last_copy = pair_copy(entering.at[0], entering.at[1], 1)
    last_copy.start()
    last_copy.wait()
    other = entering[1].astype(F32)
    state_f = jnp.where(core == 0, state, other)
    state_b = jnp.where(core == 0, other, state)
    entry = jnp.concatenate([spread(state_f, same_head), spread(state_b, same_head)], axis=1)
    mixed = out_f + out_b + low(jnp.concatenate([resp_f, resp_b], axis=1), entry, LANES)

    centred = mixed - by_head(mixed) * (1.0 / HEAD_DIM)
    scaled = centred * lax.rsqrt(by_head(centred * centred) * (1.0 / HEAD_DIM) + 0.00064)
    mix = (scaled * head_scale_ref[...] * sigmoid(out_gate_ref[...].astype(F32))).astype(BF16)
    for o in range(TP):
        mix_out[o] = mix[o * count : (o + 1) * count]

    def mix_copy(o):
        return tp_copy(mix_out.at[lax.rem(tp + o, TP)], mixes.at[tp], mix_send, mix_recv, o, o)

    for o in (2, 1, 3):
        mix_copy(o).start()
    mixes[tp] = mix_out[tp]
    for o in range(1, TP):
        give_copy(o).wait_recv()
    residual = residual_ref[...].astype(F32)
    for o in (1, 3, 2):
        mix_copy(o).wait_recv()
    wide = jnp.concatenate([mixes[o] for o in range(TP)], axis=1)
    hidden = residual + dot(wide, mixer_w[...].reshape(TP * n, width))
    hidden = hidden.astype(BF16).astype(F32)
    normed = (
        hidden * lax.rsqrt(jnp.mean(hidden * hidden, axis=1, keepdims=True) + 1e-06) * expert_scale_ref[...]
    ).astype(BF16)

    quarters = jnp.concatenate([normed[:, q * quarter : (q + 1) * quarter] for q in range(QUARTERS)], axis=0)
    packed[...] = dot(place[...], quarters).astype(BF16)
    each(out_copy, begin)
    arrived[size - piece :] = packed[size - piece :]

    each(meta_copy, arrive)
    told = meta_in[...].reshape(SP, 128)
    lane = iota((chunk, 128), 1)
    slot_lane = (iota((chunk, 128), 0) & 3) * (2 * GROUP)
    cols = QUARTERS * TP * taken
    row, col = iota((chunk, cols), 0), iota((chunk, cols), 1)
    col_q, col_o = lax.div(col, TP * taken), lax.rem(lax.div(col, taken), TP)
    col_k, col_e = lax.rem(lax.div(col, CAP), group_slots), (col & 1) + 1
    same_place = ((row >> 4) == col_k) & (((row >> 2) & 3) == col_q)
    source_row, source_col = iota((chunk, SP), 0), iota((chunk, SP), 1)
    for c in range(CHUNKS):
        widen = ((source_row >> 4) + c * group_slots == source_col).astype(F32)
        meta = dot(widen, told, precision=HIGHEST)
        codes, weights = jnp.zeros((chunk, cols), F32), jnp.zeros((chunk, cols), F32)
        for o in range(TP):
            at_code = slot_lane + lax.rem(tp + o, TP)
            code = jnp.sum(jnp.where(lane == at_code, meta, 0.0), axis=1, keepdims=True)
            weight = jnp.sum(jnp.where(lane == at_code + GROUP, meta, 0.0), axis=1, keepdims=True)
            codes, weights = jnp.where(col_o == o, code, codes), jnp.where(col_o == o, weight, weights)
        hit = same_place & (codes == col_e.astype(F32))
        pick[c] = jnp.where(hit, 1.0, 0.0).T.astype(BF16)
        weights = jnp.where(hit, weights, 0.0)
        high = weights.astype(BF16)
        weigh_hi[c] = high
        weigh_lo[c] = (weights - high.astype(F32)).astype(BF16)

    def to_expert(c, o):
        return tp_copy(outward.at[c, o], inbound.at[c, o], x_send, x_recv, c * TP + o, o)

    def from_expert(c, o):
        return tp_copy(answers.at[c, o], answered.at[c, o], y_send, y_recv, c * TP + o, TP - o)

    def take(c):
        each(out_copy, arrive, *bounds(c))
        rows = dot(pick[c], arrived[c * chunk : (c + 1) * chunk]).astype(BF16)
        for o in (2, 1, 3, 0):
            target = outward if o else inbound
            for q in range(QUARTERS):
                first = (q * TP + o) * taken
                target[c, o, :, q * quarter : (q + 1) * quarter] = rows[first : first + taken]
            if o:
                to_expert(c, o).start()

    def work(c):
        for o in (1, 3, 2):
            to_expert(c, o).wait_recv()
        rows = inbound[c].reshape(TP * taken, width)
        gate = dot(rows, gate_w[...])
        up = dot(rows, up_w[...])
        active = (gate * sigmoid(gate) * up).astype(BF16)
        result = dot(active, down_w[...]).astype(BF16)
        for o in (2, 1, 3, 0):
            target = answers if o else answered
            target[c, o] = result[o * taken : (o + 1) * taken]
            if o:
                from_expert(c, o).start()

    def give(c):
        for o in (1, 3, 2):
            from_expert(c, o).wait_recv()
        flat = answered[c].reshape(TP * taken, width)
        flat = jnp.concatenate([flat[:, q * quarter : (q + 1) * quarter] for q in range(QUARTERS)], axis=0)
        at = slice(c * chunk, (c + 1) * chunk)
        combined[at] = (dot(weigh_hi[c], flat) + dot(weigh_lo[c], flat)).astype(BF16)
        each(home_copy, begin, *bounds(c))

    for load in loads[1:]:
        load.wait()
    take(0)
    work(0)
    take(1)
    give(0)
    work(1)
    take(2)
    take(3)
    give(1)
    work(2)
    work(3)
    take(4)
    take(5)
    give(2)
    give(3)
    work(4)
    work(5)
    take(6)
    take(7)
    give(4)
    give(5)
    work(6)
    work(7)
    give(6)
    give(7)
    returned[size - piece :] = combined[size - piece :]

    for k in range(3):
        round_copy(k).wait_send()
    for k in range(4):
        scan_copy(k).wait_send()
    for o in range(1, TP):
        give_copy(o).wait_send()
        mix_copy(o).wait_send()
        for c in range(CHUNKS):
            to_expert(c, o).wait_send()
            from_expert(c, o).wait_send()
    each(meta_copy, leave)
    each(out_copy, leave)
    final = jnp.zeros((stacked, quarter), F32)
    for c in range(CHUNKS):
        each(home_copy, arrive, *bounds(c))
        at = slice(c * chunk, (c + 1) * chunk)
        final += dot(table[:, at], returned[at])
    for q in range(QUARTERS):
        at = slice(q * quarter, (q + 1) * quarter)
        updated_ref[:, at] = (hidden[:, at] + final[q * count : (q + 1) * count]).astype(BF16)

    each(home_copy, leave)


def solution(mesh):
    SP, TP = mesh.shape["sp"], mesh.shape["tp"]

    def body(
        receptance, key_matrix, value_matrix, output_gate_logits, onward_decay_logits, reverse_decay_logits,
        correction_rate_logits, extra_log_decay, documents, head_norm_scale, mixer_output_weight, residual,
        expert_norm_scale, expert_choice_index, group_route_weight, expert_route_weight,
        expert_gate_matrix, expert_up_matrix, expert_down_matrix,
    ):
        n, channels = receptance.shape
        count, width = residual.shape
        hidden_units = expert_gate_matrix.shape[2]
        piece = QUARTERS * SLOTS
        size, quarter = SP * piece, width // QUARTERS
        chunk, taken = size // CHUNKS, SP // CHUNKS * CAP
        vmem, hbm = pl.BlockSpec(memory_space=pltpu.VMEM), pl.BlockSpec(memory_space=pl.ANY)
        dma = pltpu.SemaphoreType.DMA
        return pl.pallas_call(
            functools.partial(kernel, (SP, TP)),
            out_shape=jax.ShapeDtypeStruct((count, width), BF16),
            in_specs=[vmem] * 10 + [hbm] + [vmem] * 5 + [hbm] * 3,
            out_specs=vmem,
            scratch_shapes=[
                pltpu.VMEM((2, n + 16, n), BF16),
                pltpu.VMEM((n + 16, n), BF16),
                pltpu.VMEM((4, n + 16, n), BF16),
                pltpu.VMEM((3, n + 16, n), BF16),
                pltpu.VMEM((2, n // 2 + 16, n), BF16),
                pltpu.VMEM((2, n // 2, n), BF16),
                pltpu.VMEM((TP, count, channels), BF16),
                pltpu.VMEM((TP, count, channels), BF16),
                pltpu.VMEM((SP, 1, 128), F32),
                pltpu.VMEM((SP, 1, 128), F32),
                pltpu.VMEM((size, QUARTERS * count), BF16),
                pltpu.VMEM((size, quarter), BF16),
                pltpu.VMEM((size, quarter), BF16),
                pltpu.VMEM((CHUNKS, QUARTERS * TP * taken, chunk), BF16),
                pltpu.VMEM((CHUNKS, chunk, QUARTERS * TP * taken), BF16),
                pltpu.VMEM((CHUNKS, chunk, QUARTERS * TP * taken), BF16),
                pltpu.VMEM((CHUNKS, TP, taken, width), BF16),
                pltpu.VMEM((CHUNKS, TP, taken, width), BF16),
                pltpu.VMEM((CHUNKS, TP, taken, width), BF16),
                pltpu.VMEM((CHUNKS, TP, taken, width), BF16),
                pltpu.VMEM((size, quarter), BF16),
                pltpu.VMEM((size, quarter), BF16),
                pltpu.VMEM((TP, channels, width), BF16),
                pltpu.VMEM((width, hidden_units), BF16),
                pltpu.VMEM((width, hidden_units), BF16),
                pltpu.VMEM((hidden_units, width), BF16),
                dma((4,)), dma((4,)), dma((4,)), dma((4,)), dma((3,)), dma((3,)),
                dma((TP,)), dma((TP,)), dma((TP,)), dma((TP,)), dma((SP,)), dma((SP,)), dma((SP,)), dma((SP,)),
                dma((CHUNKS * TP,)), dma((CHUNKS * TP,)), dma((CHUNKS * TP,)), dma((CHUNKS * TP,)),
                dma((SP,)), dma((SP,)),
            ],
            compiler_params=pltpu.CompilerParams(
                collective_id=0, has_side_effects=True, vmem_limit_bytes=56 * 1024 * 1024
            ),
        )(
            receptance, key_matrix, value_matrix, output_gate_logits, onward_decay_logits, reverse_decay_logits,
            correction_rate_logits, extra_log_decay.T, documents.reshape(1, n), head_norm_scale.reshape(1, channels),
            mixer_output_weight, residual, expert_norm_scale.reshape(1, width), expert_choice_index.T,
            group_route_weight.reshape(1, count), expert_route_weight.T,
            expert_gate_matrix[0], expert_up_matrix[0], expert_down_matrix[0],
        )

    in_specs = (
        (P(GRP_SP, "tp"),) * 8
        + (P(GRP_SP), P("tp"), P("tp", None), P(GRP_SP_TP, None), P(), P(GRP_SP_TP, None))
        + (P(GRP_SP_TP), P(GRP_SP_TP, None))
        + (P(SP_TP, None, None),) * 3
    )
    return jax.shard_map(
        body, mesh=mesh, in_specs=in_specs, out_specs=P(GRP_SP_TP, None), check_vma=False
    )
```
